256 devices in a mesh: ep: 64 (over z, x, core), tp: 4 (over y).
Axes of the slice: x: 4, y: 4, z: 8, core: 2. Of those that a mesh axis runs over, the one named last changes fastest.
Arguments:
- memory_query_matrix: bfloat16 [32768, 1024], P('ep', 'tp'), may hold values from -0.59765625 to 2
- memory_key_matrix: bfloat16 [32768, 1024], P('ep', 'tp'), may hold values from -0.59765625 to 2
- memory_value_matrix: bfloat16 [32768, 1024], P('ep', 'tp'), may hold values from -6 to 6
- input_gate_logits: float32 [4, 32768], P('tp', 'ep'), may hold values from -6 to 260
- forget_gate_logits: float32 [4, 32768], P('tp', 'ep'), may hold values from -1 to 20
- forget_log_boosts: float32 [4, 32768], P('tp', 'ep'), may hold values from -0.7 to 0
- head_norm_scale: float32 [1024], P('tp'), may hold values from 0.1 to 1.9
- memory_output_matrix: bfloat16 [1024, 2048], replicated, may hold values from -0.1875 to 0.1875
- projection_norm_scale: float32 [2048], replicated, may hold values from 0.1 to 1.9
- second_batch_rows: bfloat16 [49152, 2048], P(('ep', 'tp')), may hold values from -6 to 6
- expert_prenorm_scale: float32 [2048], replicated, may hold values from 0.1 to 1.9
- selected_expert_index: int32 [49152, 2], P(('ep', 'tp')), may hold values from 0 to 63, all different within a row; in each aligned block of 192 rows (0 to 191, 192 to 383, ...) at most 12 rows name the same one
- group_route_probability: float32 [49152], P(('ep', 'tp')), may hold values from 0.2 to 1
- expert_choice_scores: float32 [49152, 2], P(('ep', 'tp')), may hold values from -6 to 6
- expert_gate_matrix: bfloat16 [64, 2048, 512], P('ep'), may hold values from -0.125 to 0.125
- expert_up_matrix: bfloat16 [64, 2048, 512], P('ep'), may hold values from -0.125 to 0.125
- expert_down_matrix: bfloat16 [64, 512, 2048], P('ep'), may hold values from -0.25 to 0.25
Outputs:
- mixed_rows: bfloat16 [32768, 2048], P(('ep', 'tp'))
- routed_rows: bfloat16 [49152, 2048], P(('ep', 'tp'))
The draws below stay inside these ranges and needn't reach their ends.
Inputs may be any that keep to these rules, and one draw needn't show every extreme that they name: `selected_expert_index`: each row names 2 different experts; among the rows of one device no expert is named more than 12 times, and in some device one expert is named exactly that often.
All inputs are finite; a program needn't handle non-finite values.
Results may differ from the reference program's by a relative error of at most 0.013.
Values may be sent and summed in bfloat16 or wider, within the bound.
No kernel may reach another device: no remote copies, remote signals or barrier semaphores. Data moves between devices by JAX's collectives and lax.ppermute only.
A program may use at most 128 MiB of HBM per device.

```python
import math
import jax
import jax.numpy as jnp
import numpy as np
from jax import lax

D = 2048
HEADS = 4
HEAD_SIZE = 256
CELL_WIDTH = 1024
SPAN = 128
MIX_DEV = 512
SEQ_LEN = 32768
EXPERT_HIDDEN = 512
TOPK = 2
ROUTED_DEV = 192
ROUTED = 49152
EXPERTS = 64
CAPACITY = 12


def draw_forget_gate_logits(key, part):
    keys = jax.random.split(jax.random.fold_in(key, 71), 3)
    order = jax.random.permutation(keys[0], HEADS)
    quick = HEADS // 2
    slow_bias = math.log(SEQ_LEN) + 0.6
    bias = jnp.where(order < quick, 4.2, slow_bias).astype(jnp.float32)
    pieces = SEQ_LEN // MIX_DEV
    offset = jax.random.uniform(keys[1], (HEADS, pieces, 1), jnp.float32, -0.7, 0.7)
    offset = jnp.broadcast_to(offset, (HEADS, pieces, MIX_DEV)).reshape(HEADS, SEQ_LEN)
    noise = jnp.clip(jax.random.normal(keys[2], (HEADS, SEQ_LEN), jnp.float32), -4.0, 4.0)
    return bias[:, None] + offset + noise


def draw_forget_log_boosts(key, part):
    keys = jax.random.split(jax.random.fold_in(key, 83), 2)
    spots = jax.random.randint(keys[0], (HEADS, 3), 0, SEQ_LEN)
    depth = jax.random.uniform(keys[1], (HEADS, 3), jnp.float32, -0.69, -0.22)
    places = jnp.arange(SEQ_LEN, dtype=jnp.int32)
    hits = places[None, None, :] == spots[:, :, None]
    return jnp.min(jnp.where(hits, depth[:, :, None], 0.0), axis=1)


def draw_input_gate_logits(key, part):
    keys = jax.random.split(jax.random.fold_in(key, 97), 1)
    return jnp.clip(jax.random.normal(keys[0], (HEADS, SEQ_LEN), jnp.float32), -6.0, 6.0)


def shard_levels(stream_key, dims, shards, least, high):
    def one(dim, shards_of):
        heights = jax.random.uniform(jax.random.fold_in(jax.random.fold_in(stream_key, 6), dim), (shards_of,), jnp.float32, least / len(shards), high / len(shards))
        return jnp.repeat(jnp.exp(heights), dims[dim] // shards_of).reshape((-1,) + (1,) * (len(dims) - dim - 1))

    loudness = one(*shards[0])
    for cut in shards[1:]:
        loudness = loudness * one(*cut)
    return loudness


def shared_out(own_key, own, number, rows, count, top, most, skew):
    order = jax.random.permutation(own_key, count)
    packed, ordinary = portions_of(count, rows * top, most, skew, True), portions_of(count, rows * top, most, skew, False)
    places = jnp.arange(count)

    def named(sizes, turn):
        used = int((sizes > 0).sum())
        fixed = max(1, used // 4)
        passed = fixed + (places - fixed + turn * (used - fixed)) % max(1, count - fixed)
        return jnp.zeros((count,), jnp.int32).at[order[jnp.where(places < fixed, places, passed)]].set(jnp.asarray(sizes, jnp.int32))

    sizes = jnp.where(number % 4 == 0, named(packed, number // 4), named(ordinary, number - number // 4 - 1))
    mixed = jax.random.permutation(jax.random.fold_in(own, 3), count)
    giver, sink = mixed[0:count // 2 * 2:2], mixed[1:count // 2 * 2:2]
    slack = jnp.minimum(sizes[giver] - 1, most - sizes[sink]) // 2
    slack = jnp.where((giver == order[0]) | (sink == order[0]) | (sizes[sink] == 0), 0, jnp.maximum(slack, 0))
    passed = jax.random.randint(jax.random.fold_in(own, 4), (count // 2,), 0, 1 << 20) % (slack + 1)
    sizes = sizes.at[giver].add(-passed).at[sink].add(passed)
    items = jnp.searchsorted(jnp.cumsum(sizes), jnp.arange(rows * top), side="right").astype(jnp.int32)
    table = items.reshape(top, rows).T
    table = table[jax.random.permutation(jax.random.fold_in(own, 1), rows)]
    turn = jax.random.randint(jax.random.fold_in(own, 2), (rows, 1), 0, top)
    return jnp.take_along_axis(table, (jnp.arange(top)[None, :] + turn) % top, axis=1)


def portions_of(count, total, most, lean, full):
    portions = [(1 << 20) // math.isqrt(standing ** lean) + 1 for standing in range(1, count + 1)]
    largest = most if full else min(most, max(-(-total // count), total * portions[0] // sum(portions)))
    least = 1 if total - largest >= count - 1 else 0
    given, surplus = [largest] + [least] * (count - 1), total - largest - least * (count - 1)
    while surplus > 0:
        free = [i for i in range(1, count) if given[i] < largest] or [i for i in range(1, count) if given[i] < most]
        mass, left = sum([portions[i] for i in free]), surplus
        for i in free:
            extra = min(most - given[i], max(1, left * portions[i] // mass), surplus)
            given[i] = given[i] + extra
            surplus = surplus - extra
    return np.array(given)


def bell_draw(own_key, dims, deviation, limit, cuts=(), held_as=jnp.bfloat16):
    array = deviation * jax.random.normal(own_key, dims, jnp.float32)
    if cuts:
        array = array * shard_levels(own_key, dims, cuts, -0.22, 0.18)
    return jnp.clip(array, -limit, limit).astype(held_as)


def setup_inputs(seed: int = 0) -> dict:
    key_of = jax.random.split(jax.random.key(seed), 18)
    memory_query_matrix = jnp.clip(-0.59765625 + 2.5976562 * jax.random.uniform(key_of[0], (SEQ_LEN, CELL_WIDTH), jnp.float32) ** shard_levels(key_of[0], (SEQ_LEN, CELL_WIDTH), ((0, 64), (1, 4)), -0.2, 0.2), -0.59765625, 2.0).astype(jnp.bfloat16)
    memory_key_matrix = jnp.clip(-0.59765625 + 2.5976562 * jax.random.uniform(key_of[1], (SEQ_LEN, CELL_WIDTH), jnp.float32) ** shard_levels(key_of[1], (SEQ_LEN, CELL_WIDTH), ((0, 64), (1, 4)), -0.2, 0.2), -0.59765625, 2.0).astype(jnp.bfloat16)
    memory_value_matrix = bell_draw(key_of[2], (SEQ_LEN, CELL_WIDTH), 1.0, 6.0, ((0, 64), (1, 4)))
    input_gate_logits = draw_input_gate_logits(jax.random.fold_in(key_of[17], 71), 0)
    forget_gate_logits = draw_forget_gate_logits(jax.random.fold_in(key_of[17], 71), 0)
    forget_log_boosts = draw_forget_log_boosts(jax.random.fold_in(key_of[17], 71), 0)
    head_norm_scale = jnp.clip(1.0 + 0.18 * jax.random.normal(key_of[6], (CELL_WIDTH,), jnp.float32), 0.1, 1.9)
    memory_output_matrix = bell_draw(key_of[7], (CELL_WIDTH, D), CELL_WIDTH ** -0.5, 0.1875)
    projection_norm_scale = jnp.clip(1.0 + 0.18 * jax.random.normal(key_of[8], (D,), jnp.float32), 0.1, 1.9)
    second_batch_rows = bell_draw(key_of[9], (ROUTED, D), 1.0, 6.0, ((0, 256),))
    expert_prenorm_scale = jnp.clip(1.0 + 0.18 * jax.random.normal(key_of[10], (D,), jnp.float32), 0.1, 1.9)
    selected_expert_index_keys = jax.random.split(jax.random.fold_in(key_of[11], 1), ROUTED // ROUTED_DEV)
    selected_expert_index_turns = jax.random.permutation(jax.random.fold_in(key_of[11], 3), ROUTED // ROUTED_DEV)
    selected_expert_index = jax.vmap(lambda own, number: shared_out(jax.random.fold_in(key_of[11], 2), own, number, ROUTED_DEV, EXPERTS, TOPK, CAPACITY, 1))(selected_expert_index_keys, selected_expert_index_turns).reshape((ROUTED, TOPK))
    group_route_probability = jnp.clip(0.2 + 0.8 * jax.random.uniform(key_of[12], (ROUTED,), jnp.float32) ** shard_levels(key_of[12], (ROUTED,), ((0, 256),), -0.2, 0.2), 0.2, 1.0)
    expert_choice_scores = bell_draw(key_of[13], (ROUTED, TOPK), 1.5, 6.0, ((0, 256),), jnp.float32)
    expert_gate_matrix = bell_draw(key_of[14], (EXPERTS, D, EXPERT_HIDDEN), D ** -0.5, 0.125, ((0, 64),))
    expert_up_matrix = bell_draw(key_of[15], (EXPERTS, D, EXPERT_HIDDEN), D ** -0.5, 0.125, ((0, 64),))
    expert_down_matrix = bell_draw(key_of[16], (EXPERTS, EXPERT_HIDDEN, D), EXPERT_HIDDEN ** -0.5, 0.25, ((0, 64),))
    return dict(memory_query_matrix=memory_query_matrix, memory_key_matrix=memory_key_matrix, memory_value_matrix=memory_value_matrix, input_gate_logits=input_gate_logits, forget_gate_logits=forget_gate_logits, forget_log_boosts=forget_log_boosts, head_norm_scale=head_norm_scale, memory_output_matrix=memory_output_matrix, projection_norm_scale=projection_norm_scale, second_batch_rows=second_batch_rows, expert_prenorm_scale=expert_prenorm_scale, selected_expert_index=selected_expert_index, group_route_probability=group_route_probability, expert_choice_scores=expert_choice_scores, expert_gate_matrix=expert_gate_matrix, expert_up_matrix=expert_up_matrix, expert_down_matrix=expert_down_matrix)


floor_log = -1e+30
norm_eps = 1e-06
exact = lax.Precision.HIGHEST

def rms_scale(values, gain):
    squares = lax.optimization_barrier(jnp.mean(values * values, axis=-1, keepdims=True))
    return values * lax.rsqrt(squares + norm_eps) * gain

def span_step(carry, inputs):
    memory, normer, stabil = carry
    query, keyrow, valrow, in_gate, log_retain_factor = inputs
    key_scale = query.shape[-1] ** (-0.5)
    length = query.shape[1]
    causal = jnp.tril(jnp.ones((length, length), dtype=bool))
    cumulative = jnp.cumsum(log_retain_factor, axis=-1)
    decay_map = cumulative[:, :, None] - cumulative[:, None, :] + in_gate[:, None, :]
    decay_map = jnp.where(causal[None], decay_map, -jnp.inf)
    carried = cumulative + stabil[:, None]
    peak = jnp.maximum(carried, lax.optimization_barrier(jnp.max(decay_map, axis=-1)))
    within = jnp.exp(decay_map - peak[:, :, None])
    across = jnp.exp(carried - peak)
    qfloat = query.astype(jnp.float32)
    products = jnp.einsum('htd,hsd->hts', qfloat, keyrow.astype(jnp.float32))
    scores = products * key_scale * within
    denominator = lax.optimization_barrier(jnp.sum(scores, axis=-1)) + across * jnp.einsum('hd,htd->ht', normer, qfloat, precision=exact)
    weights = scores.astype(jnp.bfloat16)
    numerator = jnp.einsum('hts,hsd->htd', weights.astype(jnp.float32), valrow.astype(jnp.float32))
    numerator = numerator + across[:, :, None] * jnp.einsum('hed,htd->hte', memory, qfloat, precision=exact)
    output = numerator / jnp.maximum(jnp.abs(denominator), jnp.exp(-peak))[:, :, None]
    span_end = cumulative[:, -1]
    gap_log = span_end[:, None] - cumulative + in_gate
    new_peak = jnp.maximum(span_end + stabil, lax.optimization_barrier(jnp.max(gap_log, axis=-1)))
    shrink = jnp.exp(span_end + stabil - new_peak)
    spread = jnp.exp(gap_log - new_peak[:, None]) * key_scale
    keys_weighted = keyrow.astype(jnp.float32) * spread[:, :, None]
    memory = shrink[:, None, None] * memory + jnp.einsum('hse,hsd->hed', valrow.astype(jnp.float32), keys_weighted, precision=exact)
    normer = shrink[:, None] * normer + lax.optimization_barrier(jnp.sum(keys_weighted, axis=1))
    return ((memory, normer, new_peak), output)

def reference(memory_query_matrix, memory_key_matrix, memory_value_matrix, input_gate_logits, forget_gate_logits, forget_log_boosts, head_norm_scale, memory_output_matrix, projection_norm_scale, second_batch_rows, expert_prenorm_scale, selected_expert_index, group_route_probability, expert_choice_scores, expert_gate_matrix, expert_up_matrix, expert_down_matrix):
    spans = SEQ_LEN // SPAN

    def by_head(rows):
        return rows.reshape(SEQ_LEN, HEADS, HEAD_SIZE).transpose(1, 0, 2)

    def to_spans(values):
        shaped = values.reshape((HEADS, spans, SPAN) + values.shape[2:])
        return jnp.moveaxis(shaped, 1, 0)
    log_retain_factor = jax.nn.log_sigmoid(forget_gate_logits) + forget_log_boosts
    start = (jnp.zeros((HEADS, HEAD_SIZE, HEAD_SIZE), jnp.float32), jnp.zeros((HEADS, HEAD_SIZE), jnp.float32), jnp.full((HEADS,), floor_log, jnp.float32))
    inputs = (to_spans(by_head(memory_query_matrix)), to_spans(by_head(memory_key_matrix)), to_spans(by_head(memory_value_matrix)), to_spans(input_gate_logits), to_spans(log_retain_factor))
    _, cells = lax.scan(span_step, start, inputs)
    cells = jnp.moveaxis(cells, 0, 1).reshape(HEADS, SEQ_LEN, HEAD_SIZE)
    scaled = (cells * head_norm_scale.reshape(HEADS, 1, HEAD_SIZE)).astype(jnp.bfloat16)
    head_out = scaled.transpose(1, 0, 2).reshape(SEQ_LEN, CELL_WIDTH)
    projected = jnp.dot(head_out, memory_output_matrix, preferred_element_type=jnp.float32)
    mixed_rows = rms_scale(projected, projection_norm_scale).astype(jnp.bfloat16)
    ffn_rows = rms_scale(second_batch_rows.astype(jnp.float32), expert_prenorm_scale).astype(jnp.bfloat16)
    flat_ids = selected_expert_index.reshape(-1).astype(jnp.int32)
    owners = jnp.repeat(jnp.arange(ROUTED, dtype=jnp.int32), TOPK)
    onehot = (flat_ids[:, None] == jnp.arange(EXPERTS, dtype=jnp.int32)[None, :]).astype(jnp.int32)
    rank = lax.optimization_barrier(jnp.sum((jnp.cumsum(onehot, axis=0) - onehot) * onehot, axis=1)).astype(jnp.int32)
    slots = ROUTED // ROUTED_DEV * CAPACITY
    route_weight = group_route_probability[:, None] * jax.nn.softmax(expert_choice_scores, axis=-1)
    members = jnp.zeros((EXPERTS, slots), jnp.int32).at[flat_ids, rank].set(owners)
    shares = jnp.zeros((EXPERTS, slots), jnp.float32).at[flat_ids, rank].set(route_weight.reshape(-1))

    def one_expert(total, inputs):
        w_gate, w_up, w_down, member_rows, member_shares = inputs
        chosen = ffn_rows[member_rows]
        gate = jnp.dot(chosen, w_gate, preferred_element_type=jnp.float32)
        upper = jnp.dot(chosen, w_up, preferred_element_type=jnp.float32)
        hidden = (jax.nn.silu(gate) * upper).astype(jnp.bfloat16)
        answer = jnp.dot(hidden, w_down, preferred_element_type=jnp.float32).astype(jnp.bfloat16)
        total = total.at[member_rows].add(member_shares[:, None] * answer.astype(jnp.float32))
        return (total, None)
    total, _ = lax.scan(one_expert, jnp.zeros((ROUTED, D), jnp.float32), (expert_gate_matrix, expert_up_matrix, expert_down_matrix, members, shares))
    routed_rows = total.astype(jnp.bfloat16)
    return (mixed_rows, routed_rows)
```

```python
import jax
import jax.numpy as jnp
from jax import lax
from jax.experimental import pallas as pl
from jax.experimental.pallas import tpu as pltpu
from jax.sharding import Mesh
from jax.sharding import PartitionSpec as P

EP = ("ep_0", "ep_1", "ep_2")
EP_TP = ("ep_0", "ep_1", "ep_2", "tp")

floor_log = -1e30
norm_eps = 1e-06
f32, bf16, i32 = jnp.float32, jnp.bfloat16, jnp.int32


def iota(shape, dim):
    return lax.broadcasted_iota(i32, shape, dim)


def mm(a, b):
    return lax.dot_general(a, b, (((1,), (0,)), ((), ())), preferred_element_type=f32)


def mm_t(a, b):
    return lax.dot_general(a, b, (((1,), (1,)), ((), ())), preferred_element_type=f32)


def thirds(x):
    hi = x.astype(bf16).astype(f32)
    mid = (x - hi).astype(bf16).astype(f32)
    return hi, mid, (x - hi - mid).astype(bf16).astype(f32)


def halves(x):
    hi = x.astype(bf16)
    return hi, (x - hi.astype(f32)).astype(bf16)


def call(body, out_shape, *args, cost, scratch=(), specs=None, out_specs=None, grid=None, vmem=40):
    extra = {}
    if grid is not None:
        extra = dict(grid=grid, in_specs=specs, out_specs=out_specs)
    elif specs is not None:
        extra = dict(in_specs=specs)
    return pl.pallas_call(
        body,
        out_shape=out_shape,
        scratch_shapes=list(scratch),
        compiler_params=pltpu.CompilerParams(vmem_limit_bytes=vmem << 20),
        cost_estimate=pl.CostEstimate(flops=cost, bytes_accessed=cost // 500, transcendentals=0),
        **extra,
    )(*args)


def struct(shape, dtype):
    return jax.ShapeDtypeStruct(shape, dtype)


def build_body(ids, rows, gain, out, ranks):
    x = rows[...].astype(f32)
    tokens, d = x.shape
    half = d // 2
    experts = ranks.shape[0]
    mean = jnp.mean(x * x, axis=-1, keepdims=True)
    xn = (x * lax.rsqrt(mean + norm_eps) * gain[...]).astype(bf16)
    expert = iota((experts, tokens), 0)
    chosen = (ids[0:1, :] == expert) | (ids[1:2, :] == expert)
    ahead = (iota((tokens, tokens), 0) < iota((tokens, tokens), 1)).astype(f32).astype(bf16)
    count = mm(chosen.astype(f32).astype(bf16), ahead)
    rank = jnp.where(chosen, count, -1.0)
    ranks[...] = rank
    row = iota((experts, 8, tokens), 1)
    held = rank[:, None, :]

    def placing(hit):
        return hit.astype(f32).reshape(experts * 8, tokens).astype(bf16)

    out[:, :d] = mm(placing(held == row.astype(f32)), xn).astype(bf16)
    late = held == ((row & 3) + 8).astype(f32)
    first, last = placing(late & (row < 4)), placing(late & (row >= 4))
    out[:, d:] = (mm(first, xn[:, :half]) + mm(last, xn[:, half:])).astype(bf16)


def shares_body(ids, prob, scores, ranks, share8, share4):
    rank = ranks[...]
    experts, tokens = rank.shape
    s0, s1 = scores[0:1, :], scores[1:2, :]
    top = jnp.maximum(s0, s1)
    e0, e1 = jnp.exp(s0 - top), jnp.exp(s1 - top)
    both = e0 + e1
    w0, w1 = prob[...] * (e0 / both), prob[...] * (e1 / both)
    expert = iota((experts, tokens), 0)
    share = jnp.where(ids[0:1, :] == expert, w0, 0.0) + jnp.where(ids[1:2, :] == expert, w1, 0.0)
    row = iota((experts, 8, tokens), 1)

    def placed(hit, out):
        at = jnp.where(hit, share[:, None, :], 0.0).reshape(experts * 8, tokens).T
        out[:tokens], out[tokens:] = halves(at)

    placed(rank[:, None, :] == row.astype(f32), share8)
    hit = rank[:, None, :] == ((row & 3) + 8).astype(f32)
    for h in range(2):
        placed(hit & ((row >> 2) == h), share4.at[h])


def silu_mul(gate, upper):
    return (gate / (1.0 + jnp.exp(-gate)) * upper).astype(bf16)


def ffn_body(x, wg, wu, wd, out):
    d, width = wg.shape
    half = d // 2
    x8 = x[:, :d]
    hidden = silu_mul(mm(x8, wg[...]), mm(x8, wu[...]))
    out[:, :d] = mm(hidden, wd[...]).astype(bf16)
    x4 = x[:, d:]
    rows = x4.shape[0]
    first = (iota((rows, 1), 0) & 4) == 0

    def joined(w):
        z = jnp.where(first, mm(x4, w[:half, :]), mm(x4, w[half:, :]))
        z3 = z.reshape(rows // 8, 8, width)
        return (z3 + pltpu.roll(z3, 4, 1)).reshape(rows, width)

    hidden = silu_mul(joined(wg), joined(wu))
    out[:, d:] = jnp.where(first, mm(hidden, wd[:, :half]), mm(hidden, wd[:, half:])).astype(bf16)


def combine_body(share8, share4, back, out):
    tokens, d = out.shape
    half = d // 2
    late = back[:, d:]
    for h in range(2):
        cols = slice(h * half, (h + 1) * half)
        total = mm(share8[...], back[:, cols]) + mm(share4[h], late)
        out[:, cols] = (total[:tokens] + total[tokens:]).astype(bf16)


def running_keep(forget, boosts):
    x = forget[...]
    keep = boosts[...] - (jnp.maximum(-x, 0.0) + jnp.log1p(jnp.exp(-jnp.abs(x))))
    length = keep.shape[1]
    pieces = jnp.concatenate([*thirds(keep), jnp.zeros((5, length), f32)], axis=0).astype(bf16)
    upto = (iota((length, length), 0) <= iota((length, length), 1)).astype(f32).astype(bf16)
    return jnp.sum(mm(pieces, upto), axis=0, keepdims=True)


def side_rows(normer, total, peak):
    width = normer.shape[1]
    hi = normer.astype(bf16).astype(f32)
    lane = iota((1, width), 1)
    info = jnp.zeros((1, width), f32)
    for at, piece in enumerate((*thirds(total), *thirds(peak))):
        info = jnp.where(lane == at, piece, info)
    return jnp.concatenate([hi, normer - hi, info, jnp.zeros((5, width), f32)], axis=0)


def read_side(side):
    normer = side[0:1, :] + side[1:2, :]
    info = side[2:3, :]
    total = info[:, 0:1] + info[:, 1:2] + info[:, 2:3]
    peak = info[:, 3:4] + info[:, 4:5] + info[:, 5:6]
    return normer, total, peak


def summary_body(keys, values, gates, forget, boosts, out):
    b = running_keep(forget, boosts)
    length = b.shape[1]
    width = keys.shape[1]
    last = b[:, length - 1 : length]
    gap = last - b + gates[...]
    peak = jnp.max(gap, axis=1, keepdims=True)
    spread = jnp.exp(gap - peak) * (width**-0.5)
    k = keys[...]
    scaled = (values[...].astype(f32).T * spread).astype(bf16)
    out[:width, :] = mm(scaled, k).astype(bf16)
    hi, lo = halves(spread)
    two = jnp.concatenate([hi.astype(f32), lo.astype(f32), jnp.zeros((6, length), f32)], axis=0)
    normer = jnp.sum(mm(two.astype(bf16), k), axis=0, keepdims=True)
    out[width:, :] = side_rows(normer, last, peak).astype(bf16)


def weighted(pieces, logs, floor):
    stabil = floor
    for level in logs:
        stabil = jnp.maximum(stabil, level)
    memory, normer = None, None
    for (piece, n), level in zip(pieces, logs):
        factor = jnp.exp(level - stabil)
        memory = factor * piece if memory is None else memory + factor * piece
        normer = factor * n if normer is None else normer + factor * n
    return memory, normer, stabil


def before(mine, totals, peaks):
    logs, kept = [], []
    floor = jnp.full((1, 1), floor_log, f32)
    for j in range(len(totals)):
        level = peaks[j]
        for l in range(j + 1, len(totals)):
            level = level + jnp.where(l < mine, totals[l], 0.0)
        kept.append(j < mine)
        logs.append(jnp.where(j < mine, level, floor))
    return logs, kept


def masked(kept, pieces):
    return [(jnp.where(k, c, 0.0), jnp.where(k, n, 0.0)) for k, (c, n) in zip(kept, pieces)]


def plane_body(where, got, out, own, small, whole_memory):
    mine = where[1]
    width = got.shape[2]
    count = got.shape[0]
    pieces, totals, peaks = [], [], []
    for j in range(count):
        normer, total, peak = read_side(got[j, width:, :].astype(f32))
        pieces.append((got[j, :width, :].astype(f32), normer))
        totals.append(total)
        peaks.append(peak)
    logs = []
    for j in range(count):
        level = peaks[j]
        for l in range(j + 1, count):
            level = level + totals[l]
        logs.append(level)
    memory, normer, stabil = weighted(pieces, logs, logs[0])
    everything = totals[0]
    for total in totals[1:]:
        everything = everything + total
    whole_memory[...] = memory
    part = width // count
    out[:part, :] = whole_memory[pl.ds(pl.multiple_of(mine * part, 8), part), :].astype(bf16)
    out[part:, :] = side_rows(normer, everything, stabil).astype(bf16)
    logs, kept = before(mine, totals, peaks)
    memory, normer, stabil = weighted(
        masked(kept, pieces), logs, jnp.full((1, 1), floor_log, f32)
    )
    own[...] = memory
    passed = jnp.zeros((1, 1), f32)
    for l in range(count):
        passed = passed + jnp.where(l < mine, totals[l], 0.0)
    small[0:1, :] = normer
    small[1:2, :] = jnp.broadcast_to(stabil, (1, width))
    small[2:3, :] = jnp.broadcast_to(passed, (1, width))
    small[3:8, :] = jnp.zeros((5, width), f32)


def line_body(where, got, out, small):
    mine = where[0]
    part = out.shape[0]
    width = got.shape[2]
    pieces, totals, peaks = [], [], []
    for j in range(got.shape[0]):
        normer, total, peak = read_side(got[j, part:, :].astype(f32))
        pieces.append((got[j, :part, :].astype(f32), normer))
        totals.append(total)
        peaks.append(peak)
    logs, kept = before(mine, totals, peaks)
    memory, normer, stabil = weighted(
        masked(kept, pieces), logs, jnp.full((1, 1), floor_log, f32)
    )
    out[...] = memory.astype(bf16)
    small[0:1, :] = normer
    small[1:2, :] = jnp.broadcast_to(stabil, (1, width))
    small[2:8, :] = jnp.zeros((6, width), f32)


def cell_body(query, keys, values, gates, forget, boosts, state, line, own, near, scale, out):
    b = running_keep(forget, boosts)
    length = b.shape[1]
    width = keys.shape[1]
    b_col = jnp.broadcast_to(b, (128, length)).T
    far_log = near[2:3, 0:1] + line[1:2, 0:1]
    near_log = near[1:2, 0:1]
    stabil = jnp.maximum(far_log, near_log)
    far, close = jnp.exp(far_log - stabil), jnp.exp(near_log - stabil)
    normer = far * line[0:1, :] + close * near[0:1, :]
    memory = (far * state[...].astype(f32) + close * own[...]).astype(bf16)
    source = gates[...] - b
    block = 128
    for start in range(0, length, block):
        upto = start + block
        rows = slice(start, upto)
        q = query[rows, :]
        bt = b_col[rows, 0:1]
        decay = bt + source[:, :upto]
        seen = iota((block, upto), 1) <= iota((block, upto), 0) + start
        decay = jnp.where(seen, decay, -jnp.inf)
        carried = bt + stabil
        peak = jnp.maximum(carried, jnp.max(decay, axis=1, keepdims=True))
        across = jnp.exp(carried - peak)
        scores = mm_t(q, keys[:upto, :]) * (width**-0.5) * jnp.exp(decay - peak)
        den = jnp.sum(scores, axis=1, keepdims=True) + across * jnp.sum(
            q.astype(f32) * normer, axis=1, keepdims=True
        )
        num = mm(scores.astype(bf16), values[:upto, :]) + across * mm_t(q, memory)
        cell = num / jnp.maximum(jnp.abs(den), jnp.exp(-peak))
        out[rows, :] = (cell * scale[...]).astype(bf16)


def project_body(where, *refs):
    heads, (weight, gain, out) = refs[:-3], refs[-3:]
    count = len(heads)
    width = heads[0].shape[-1]
    total = None
    for step, head in enumerate(heads):
        source = lax.rem(where[2] + count - step, count)
        rows = weight[pl.ds(pl.multiple_of(source * width, width), width), :]
        product = mm(head[...], rows)
        total = product if total is None else total + product
    mean = jnp.mean(total * total, axis=-1, keepdims=True)
    out[...] = (total * lax.rsqrt(mean + norm_eps) * gain[...]).astype(bf16)


def exchanged(array, axes):
    return lax.all_to_all(array, axes, split_axis=0, concat_axis=0, tiled=True)


def after(array, *earlier):
    return lax.optimization_barrier((array, *earlier))[0]


def shards(
    query,
    keys,
    values,
    in_gates,
    forget,
    boosts,
    head_scale,
    out_weight,
    out_gain,
    rows,
    row_gain,
    ids,
    prob,
    scores,
    w_gate,
    w_up,
    w_down,
):
    devices = lax.axis_size(EP)
    positions, width = query.shape
    tokens, d = rows.shape
    hidden = w_gate.shape[2]
    slots = devices * 8
    plane = lax.axis_size(("ep_1", "ep_2"))
    planes = lax.axis_size("tp")
    wg, wu, wd = w_gate[0], w_up[0], w_down[0]
    ids_t = ids.T
    vm = pl.BlockSpec(memory_space=pltpu.VMEM)
    sm = pl.BlockSpec(memory_space=pltpu.SMEM)
    where = jnp.stack(
        [lax.axis_index("ep_0"), lax.axis_index(("ep_1", "ep_2")), lax.axis_index("tp")]
    ).astype(i32)

    out, ranks = call(
        build_body,
        (struct((slots, d + d // 2), bf16), struct((devices, tokens), f32)),
        ids_t,
        rows,
        row_gain.reshape(1, d),
        cost=4 * slots * tokens * d,
    )
    got = exchanged(out.reshape(devices, 8, d + d // 2), EP)
    send = call(
        summary_body,
        struct((width + 8, width), bf16),
        after(keys, out),
        values,
        in_gates,
        forget,
        boosts,
        cost=2 * positions * width * width * 4,
    )
    states = lax.all_gather(send, ("ep_1", "ep_2"))
    send, own, near = call(
        plane_body,
        (
            struct((width // plane + 8, width), bf16),
            struct((width, width), f32),
            struct((8, width), f32),
        ),
        where,
        states,
        cost=4 * plane * width * width * 100,
        scratch=(pltpu.VMEM((width, width), f32),),
        specs=[sm, vm],
    )
    states = lax.all_gather(send, "ep_0")
    send, far = call(
        line_body,
        (struct((width // plane, width), bf16), struct((8, width), f32)),
        where,
        states,
        cost=4 * width * width * 100,
        specs=[sm, vm],
    )
    share8, share4 = call(
        shares_body,
        (struct((2 * tokens, slots), bf16), struct((2, 2 * tokens, slots), bf16)),
        ids_t,
        prob.reshape(1, tokens),
        scores.T,
        after(ranks, out),
        cost=slots * tokens * 1000,
    )
    block = 128
    answers = call(
        ffn_body,
        struct((slots, d + d // 2), bf16),
        got.reshape(slots, d + d // 2),
        wg,
        wu,
        wd,
        cost=12 * slots * d * hidden,
        grid=(slots // block,),
        specs=[pl.BlockSpec((block, d + d // 2), lambda i: (i, 0)), vm, vm, vm],
        out_specs=pl.BlockSpec((block, d + d // 2), lambda i: (i, 0)),
    )
    back = exchanged(answers.reshape(devices, 8, d + d // 2), EP)
    state = lax.all_gather(send, ("ep_1", "ep_2"), tiled=True)
    heads = call(
        cell_body,
        struct((positions, width), bf16),
        query,
        keys,
        values,
        in_gates,
        forget,
        boosts,
        state,
        far,
        own,
        near,
        head_scale.reshape(1, width),
        cost=2 * positions * positions * width * 40,
    )
    share = positions // planes
    me = where[2]
    pieces = []
    for step in range(planes):
        first = lax.rem(me + step, planes) * share
        piece = lax.dynamic_slice_in_dim(heads, first, share, 0)
        if step:
            ring = [(i, (i + step) % planes) for i in range(planes)]
            piece = lax.ppermute(piece, "tp", ring)
        pieces.append(piece)
    mixed_rows = call(
        project_body,
        struct((share, d), bf16),
        where,
        *pieces,
        out_weight,
        out_gain.reshape(1, d),
        cost=20 * positions * width * d,
        specs=[sm] + [vm] * (planes + 2),
    )
    routed_rows = call(
        combine_body,
        struct((tokens, d), bf16),
        share8,
        share4,
        back.reshape(slots, d + d // 2),
        cost=12 * tokens * slots * d,
    )
    return (mixed_rows, routed_rows)


def solution(mesh):
    finer = Mesh(mesh.devices.reshape(8, 4, 2, mesh.shape["tp"]), ("ep_0", "ep_1", "ep_2", "tp"))
    in_specs = (
        P(EP, "tp"),
        P(EP, "tp"),
        P(EP, "tp"),
        P("tp", EP),
        P("tp", EP),
        P("tp", EP),
        P("tp"),
        P(),
        P(),
        P(EP_TP, None),
        P(),
        P(EP_TP, None),
        P(EP_TP),
        P(EP_TP, None),
        P(EP, None, None),
        P(EP, None, None),
        P(EP, None, None),
    )
    out_specs = (P(EP_TP, None), P(EP_TP, None))
    return jax.shard_map(
        shards, mesh=finer, in_specs=in_specs, out_specs=out_specs, check_vma=False
    )
```

```python
import jax
import jax.numpy as jnp
from jax import lax
from jax.experimental import pallas as pl
from jax.experimental.pallas import tpu as pltpu
from jax.sharding import Mesh
from jax.sharding import PartitionSpec as P

EP = ("ep_0", "ep_1", "ep_2")
EP_TP = ("ep_0", "ep_1", "ep_2", "tp")


floor_log = -1e30
norm_eps = 1e-06
f32, bf16, i32 = jnp.float32, jnp.bfloat16, jnp.int32


def iota(shape, dim):
    return lax.broadcasted_iota(i32, shape, dim)


def mm(a, b):
    return lax.dot_general(a, b, (((1,), (0,)), ((), ())), preferred_element_type=f32)


def mm_t(a, b):
    return lax.dot_general(a, b, (((1,), (1,)), ((), ())), preferred_element_type=f32)


def thirds(x):
    hi = x.astype(bf16).astype(f32)
    mid = (x - hi).astype(bf16).astype(f32)
    return hi, mid, (x - hi - mid).astype(bf16).astype(f32)


def halves(x):
    hi = x.astype(bf16)
    return hi, (x - hi.astype(f32)).astype(bf16)


def whole(*shape):
    return pl.BlockSpec(shape, lambda *_: (0,) * len(shape))


def call(body, out_shape, *args, cost, scratch=(), specs=None, out_specs=None, grid=None, vmem=24):
    extra = {}
    if grid is not None:
        extra = dict(grid=grid, in_specs=specs, out_specs=out_specs)
    elif specs is not None:
        extra = dict(in_specs=specs)
        if out_specs is not None:
            extra["out_specs"] = out_specs
    return pl.pallas_call(
        body,
        out_shape=out_shape,
        scratch_shapes=list(scratch),
        compiler_params=pltpu.CompilerParams(vmem_limit_bytes=vmem << 20),
        cost_estimate=pl.CostEstimate(flops=cost, bytes_accessed=cost // 500, transcendentals=0),
        **extra,
    )(*args)


def struct(shape, dtype):
    return jax.ShapeDtypeStruct(shape, dtype)


def build_body(ids, rows, gain, out, ranks, normed, held):
    d = rows.shape[1]
    half = d // 2
    experts, tokens = ranks.shape

    @pl.when(pl.program_id(0) == 0)
    def _():
        x = rows[...].astype(f32)
        mean = jnp.mean(x * x, axis=-1, keepdims=True)
        normed[...] = (x * lax.rsqrt(mean + norm_eps) * gain[...]).astype(bf16)
        expert = iota((experts, tokens), 0)
        chosen = (ids[0:1, :] == expert) | (ids[1:2, :] == expert)
        ahead = (iota((tokens, tokens), 0) < iota((tokens, tokens), 1)).astype(f32).astype(bf16)
        count = mm(chosen.astype(f32).astype(bf16), ahead)
        rank = jnp.where(chosen, count, -1.0)
        ranks[...] = rank
        held[...] = rank

    part = out.shape[0] // 8
    first_expert = pl.multiple_of(pl.program_id(0) * part, 8)
    rank = held[pl.ds(first_expert, part), :][:, None, :]
    row = iota((part, 8, tokens), 1)

    def placing(hit):
        return hit.astype(f32).reshape(part * 8, tokens).astype(bf16)

    out[:, :d] = mm(placing(rank == row.astype(f32)), normed[...]).astype(bf16)
    late = rank == ((row & 3) + 8).astype(f32)
    first, last = placing(late & (row < 4)), placing(late & (row >= 4))
    out[:, d:] = (mm(first, normed[:, :half]) + mm(last, normed[:, half:])).astype(bf16)


def shares_body(ids, prob, scores, ranks, share8, share4):
    rank = ranks[...]
    experts, tokens = rank.shape
    s0, s1 = scores[0:1, :], scores[1:2, :]
    top = jnp.maximum(s0, s1)
    e0, e1 = jnp.exp(s0 - top), jnp.exp(s1 - top)
    both = e0 + e1
    w0, w1 = prob[...] * (e0 / both), prob[...] * (e1 / both)
    expert = iota((experts, tokens), 0)
    share = jnp.where(ids[0:1, :] == expert, w0, 0.0) + jnp.where(ids[1:2, :] == expert, w1, 0.0)
    row = iota((experts, 8, tokens), 1)

    def placed(hit, out):
        at = jnp.where(hit, share[:, None, :], 0.0).reshape(experts * 8, tokens).T
        out[:tokens], out[tokens:] = halves(at)

    placed(rank[:, None, :] == row.astype(f32), share8)
    hit = rank[:, None, :] == ((row & 3) + 8).astype(f32)
    for h in range(2):
        placed(hit & ((row >> 2) == h), share4.at[h])


def silu_mul(gate, upper):
    return (gate / (1.0 + jnp.exp(-gate)) * upper).astype(bf16)


def ffn_body(x_far, wg_far, wu_far, wd_far, out, x, wg, wu, wd, made, sems, x_sems, out_sems):
    d, width = wg.shape
    half = d // 2
    loads = [
        pltpu.make_async_copy(far, near, sems.at[k])
        for k, (far, near) in enumerate(((wg_far, wg), (wu_far, wu), (wd_far, wd)))
    ]
    block = made.shape[1]
    steps = out.shape[0] // block
    arrivals = [
        pltpu.make_async_copy(
            x_far.at[pl.ds(step * block, block), :],
            x.at[pl.ds(step * block, block), :],
            x_sems.at[step],
        )
        for step in range(steps)
    ]
    for load in (arrivals[0], *loads, *arrivals[1:]):
        load.start()
    first = (iota((block, 1), 0) & 4) == 0

    def joined(x4, w):
        z = jnp.where(first, mm(x4, w[:half, :]), mm(x4, w[half:, :]))
        z3 = z.reshape(block // 8, 8, width)
        return (z3 + pltpu.roll(z3, 4, 1)).reshape(block, width)

    def store(step):
        return pltpu.make_async_copy(
            made.at[step], out.at[pl.ds(step * block, block), :], out_sems.at[step]
        )

    for step in range(steps):
        rows = slice(step * block, (step + 1) * block)
        arrivals[step].wait()
        x8, x4 = x[rows, :d], x[rows, d:]
        if step == 0:
            loads[0].wait()
        gate8, gate4 = mm(x8, wg[...]), joined(x4, wg)
        if step == 0:
            loads[1].wait()
        hidden8 = silu_mul(gate8, mm(x8, wu[...]))
        hidden4 = silu_mul(gate4, joined(x4, wu))
        if step == 0:
            loads[2].wait()
        made[step, :, :d] = mm(hidden8, wd[...]).astype(bf16)
        made[step, :, d:] = jnp.where(
            first, mm(hidden4, wd[:, :half]), mm(hidden4, wd[:, half:])
        ).astype(bf16)
        store(step).start()
    for step in range(steps):
        store(step).wait()


def combine_body(share8, share4, early, late, out):
    tokens = out.shape[0]
    total = mm(share8[...], early[...]) + mm(share4[0], late[...])
    out[...] = (total[:tokens] + total[tokens:]).astype(bf16)


def running_keep(forget, boosts):
    x = forget[...]
    keep = boosts[...] - (jnp.maximum(-x, 0.0) + jnp.log1p(jnp.exp(-jnp.abs(x))))
    length = keep.shape[1]
    pieces = jnp.concatenate([*thirds(keep), jnp.zeros((5, length), f32)], axis=0).astype(bf16)
    upto = (iota((length, length), 0) <= iota((length, length), 1)).astype(f32).astype(bf16)
    return jnp.sum(mm(pieces, upto), axis=0, keepdims=True)


def side_rows(normer, total, peak):
    width = normer.shape[1]
    hi = normer.astype(bf16).astype(f32)
    lane = iota((1, width), 1)
    info = jnp.zeros((1, width), f32)
    for at, piece in enumerate((*thirds(total), *thirds(peak))):
        info = jnp.where(lane == at, piece, info)
    return jnp.concatenate([hi, normer - hi, info, jnp.zeros((5, width), f32)], axis=0)


def read_side(side):
    normer = side[0:1, :] + side[1:2, :]
    info = side[2:3, :]
    total = info[:, 0:1] + info[:, 1:2] + info[:, 2:3]
    peak = info[:, 3:4] + info[:, 4:5] + info[:, 5:6]
    return normer, total, peak


def summary_body(keys, values, gates, forget, boosts, out, rest):
    b = running_keep(forget, boosts)
    length = b.shape[1]
    width = keys.shape[1]
    last = b[:, length - 1 : length]
    gap = last - b + gates[...]
    peak = jnp.max(gap, axis=1, keepdims=True)
    spread = jnp.exp(gap - peak) * (width**-0.5)
    k = keys[...]
    scaled = (values[...].astype(f32).T * spread).astype(bf16)
    half = width // 2
    memory = mm(scaled, k).astype(bf16)
    out[:half, :] = memory[:half]
    rest[...] = memory[half:]
    hi, lo = halves(spread)
    two = jnp.concatenate([hi.astype(f32), lo.astype(f32), jnp.zeros((6, length), f32)], axis=0)
    normer = jnp.sum(mm(two.astype(bf16), k), axis=0, keepdims=True)
    out[half:, :] = side_rows(normer, last, peak).astype(bf16)


def weighted(pieces, logs, floor):
    stabil = floor
    for level in logs:
        stabil = jnp.maximum(stabil, level)
    memory, normer = None, None
    for (piece, n), level in zip(pieces, logs):
        factor = jnp.exp(level - stabil)
        memory = factor * piece if memory is None else memory + factor * piece
        normer = factor * n if normer is None else normer + factor * n
    return memory, normer, stabil


def before(mine, totals, peaks):
    logs, kept = [], []
    floor = jnp.full((1, 1), floor_log, f32)
    for j in range(len(totals)):
        level = peaks[j]
        for l in range(j + 1, len(totals)):
            level = level + jnp.where(l < mine, totals[l], 0.0)
        kept.append(j < mine)
        logs.append(jnp.where(j < mine, level, floor))
    return logs, kept


def masked(kept, pieces):
    return [(jnp.where(k, c, 0.0), jnp.where(k, n, 0.0)) for k, (c, n) in zip(kept, pieces)]


def plane_body(where, got, more, out, own, small, whole_memory):
    mine = where[1]
    width = got.shape[2]
    half = width // 2
    count = got.shape[0]
    pieces, totals, peaks = [], [], []
    for j in range(count):
        normer, total, peak = read_side(got[j, half:, :].astype(f32))
        memory = jnp.concatenate([got[j, :half, :], more[j]], axis=0).astype(f32)
        pieces.append((memory, normer))
        totals.append(total)
        peaks.append(peak)
    logs = []
    for j in range(count):
        level = peaks[j]
        for l in range(j + 1, count):
            level = level + totals[l]
        logs.append(level)
    memory, normer, stabil = weighted(pieces, logs, logs[0])
    everything = totals[0]
    for total in totals[1:]:
        everything = everything + total
    whole_memory[...] = memory
    part = width // count
    out[:part, :] = whole_memory[pl.ds(pl.multiple_of(mine * part, 8), part), :].astype(bf16)
    out[part:, :] = side_rows(normer, everything, stabil).astype(bf16)
    logs, kept = before(mine, totals, peaks)
    memory, normer, stabil = weighted(
        masked(kept, pieces), logs, jnp.full((1, 1), floor_log, f32)
    )
    own[...] = memory
    passed = jnp.zeros((1, 1), f32)
    for l in range(count):
        passed = passed + jnp.where(l < mine, totals[l], 0.0)
    small[0:1, :] = normer
    small[1:2, :] = jnp.broadcast_to(stabil, (1, width))
    small[2:3, :] = jnp.broadcast_to(passed, (1, width))
    small[3:8, :] = jnp.zeros((5, width), f32)


def line_body(where, *refs):
    got, (out, small) = refs[:-2], refs[-2:]
    mine = where[0]
    part, width = out.shape
    floor = jnp.full((1, 1), floor_log, f32)
    passed = jnp.zeros((1, 1), f32)
    pieces, logs, kept = [], [], []
    for step, piece in enumerate(got):
        normer, total, peak = read_side(piece[part:, :].astype(f32))
        near = step < mine
        pieces.append((piece[:part, :].astype(f32), normer))
        logs.append(jnp.where(near, peak + passed, floor))
        kept.append(near)
        passed = passed + jnp.where(near, total, 0.0)
    memory, normer, stabil = weighted(masked(kept, pieces), logs, floor)
    out[...] = memory.astype(bf16)
    small[0:1, :] = normer
    small[1:2, :] = jnp.broadcast_to(stabil, (1, width))
    small[2:8, :] = jnp.zeros((6, width), f32)


def cell_body(query, keys, values, gates, forget, boosts, state, line, own, near, scale, out):
    b = running_keep(forget, boosts)
    length = b.shape[1]
    width = keys.shape[1]
    b_col = jnp.broadcast_to(b, (128, length)).T
    far_log = near[2:3, 0:1] + line[1:2, 0:1]
    near_log = near[1:2, 0:1]
    stabil = jnp.maximum(far_log, near_log)
    far, close = jnp.exp(far_log - stabil), jnp.exp(near_log - stabil)
    normer = far * line[0:1, :] + close * near[0:1, :]
    memory = (far * state[...].astype(f32) + close * own[...]).astype(bf16)
    source = gates[...] - b
    block = 128
    for start in range(0, length, block):
        upto = start + block
        rows = slice(start, upto)
        q = query[rows, :]
        bt = b_col[rows, 0:1]
        decay = bt + source[:, :upto]
        seen = iota((block, upto), 1) <= iota((block, upto), 0) + start
        decay = jnp.where(seen, decay, -jnp.inf)
        carried = bt + stabil
        peak = jnp.maximum(carried, jnp.max(decay, axis=1, keepdims=True))
        across = jnp.exp(carried - peak)
        scores = mm_t(q, keys[:upto, :]) * (width**-0.5) * jnp.exp(decay - peak)
        den = jnp.sum(scores, axis=1, keepdims=True) + across * jnp.sum(
            q.astype(f32) * normer, axis=1, keepdims=True
        )
        num = mm(scores.astype(bf16), values[:upto, :]) + across * mm_t(q, memory)
        cell = num / jnp.maximum(jnp.abs(den), jnp.exp(-peak))
        out[rows, :] = (cell * scale[...]).astype(bf16)


def project_body(where, *refs):
    heads, (weight, gain, out) = refs[:-3], refs[-3:]
    count = len(heads)
    width = heads[0].shape[-1]
    total = None
    for step, head in enumerate(heads):
        source = lax.rem(where[2] + count - step, count)
        rows = weight[pl.ds(pl.multiple_of(source * width, width), width), :]
        product = mm(head[...], rows)
        total = product if total is None else total + product
    mean = jnp.mean(total * total, axis=-1, keepdims=True)
    out[...] = (total * lax.rsqrt(mean + norm_eps) * gain[...]).astype(bf16)


def exchanged(array, axes):
    return lax.all_to_all(array, axes, split_axis=0, concat_axis=0, tiled=True)


def after(array, *earlier):
    return lax.optimization_barrier((array, *earlier))[0]


def shards(
    query,
    keys,
    values,
    in_gates,
    forget,
    boosts,
    head_scale,
    out_weight,
    out_gain,
    rows,
    row_gain,
    ids,
    prob,
    scores,
    w_gate,
    w_up,
    w_down,
):
    devices = lax.axis_size(EP)
    positions, width = query.shape
    tokens, d = rows.shape
    hidden = w_gate.shape[2]
    slots = devices * 8
    line, plane = lax.axis_size("ep_0"), lax.axis_size(("ep_1", "ep_2"))
    planes = lax.axis_size("tp")
    wg, wu, wd = w_gate[0], w_up[0], w_down[0]
    ids_t = ids.T
    vm = pl.BlockSpec(memory_space=pltpu.VMEM)
    sm = pl.BlockSpec(memory_space=pltpu.SMEM)
    far_away = pl.BlockSpec(memory_space=pltpu.HBM)
    where = jnp.stack(
        [lax.axis_index("ep_0"), lax.axis_index(("ep_1", "ep_2")), lax.axis_index("tp")]
    ).astype(i32)

    out, ranks = call(
        build_body,
        (struct((slots, d + d // 2), bf16), struct((devices, tokens), f32)),
        ids_t,
        rows,
        row_gain.reshape(1, d),
        cost=4 * slots * tokens * d,
        grid=(4,),
        specs=[whole(2, tokens), whole(tokens, d), whole(1, d)],
        out_specs=(
            pl.BlockSpec((slots // 4, d + d // 2), lambda i: (i, 0)),
            whole(devices, tokens),
        ),
        scratch=(pltpu.VMEM((tokens, d), bf16), pltpu.VMEM((devices, tokens), f32)),
        vmem=60,
    )
    got = exchanged(out.reshape(devices, 8, d + d // 2), EP)
    send, rest = call(
        summary_body,
        (struct((width // 2 + 8, width), bf16), struct((width // 2, width), bf16)),
        after(keys, out),
        values,
        in_gates,
        forget,
        boosts,
        cost=2 * positions * width * width * 4,
    )
    states = lax.all_gather(send, ("ep_1", "ep_2"))
    more = lax.all_gather(after(rest, states), ("ep_1", "ep_2"))
    send, own, near = call(
        plane_body,
        (
            struct((width // plane + 8, width), bf16),
            struct((width, width), f32),
            struct((8, width), f32),
        ),
        where,
        states,
        more,
        cost=4 * plane * width * width * 100,
        scratch=(pltpu.VMEM((width, width), f32),),
        specs=[sm, vm, vm],
    )
    states = [
        lax.ppermute(send, "ep_0", [(i, i + step) for i in range(line - step)])
        for step in range(1, line)
    ]
    send, far = call(
        line_body,
        (struct((width // plane, width), bf16), struct((8, width), f32)),
        where,
        *states,
        cost=4 * width * width * 100,
        specs=[sm] + [vm] * (line - 1),
    )
    share8, share4 = call(
        shares_body,
        (struct((2 * tokens, slots), bf16), struct((2, 2 * tokens, slots), bf16)),
        ids_t,
        prob.reshape(1, tokens),
        scores.T,
        after(ranks, out),
        cost=slots * tokens * 1000,
    )
    block = 128
    answers = call(
        ffn_body,
        struct((slots, d + d // 2), bf16),
        after(got, send).reshape(slots, d + d // 2),
        wg,
        wu,
        wd,
        cost=12 * slots * d * hidden,
        specs=[far_away] * 4,
        out_specs=far_away,
        scratch=(
            pltpu.VMEM((slots, d + d // 2), bf16),
            pltpu.VMEM((d, hidden), bf16),
            pltpu.VMEM((d, hidden), bf16),
            pltpu.VMEM((hidden, d), bf16),
            pltpu.VMEM((slots // block, block, d + d // 2), bf16),
            pltpu.SemaphoreType.DMA((3,)),
            pltpu.SemaphoreType.DMA((slots // block,)),
            pltpu.SemaphoreType.DMA((slots // block,)),
        ),
        vmem=50,
    )
    back = exchanged(answers.reshape(devices, 8, d + d // 2), EP)
    state = lax.all_gather(send, ("ep_1", "ep_2"), tiled=True)
    heads = call(
        cell_body,
        struct((positions, width), bf16),
        query,
        keys,
        values,
        in_gates,
        forget,
        boosts,
        state,
        far,
        own,
        near,
        head_scale.reshape(1, width),
        cost=2 * positions * positions * width * 40,
    )
    share = positions // planes
    me = where[2]
    pieces = []
    for step in range(planes):
        first = lax.rem(me + step, planes) * share
        piece = lax.dynamic_slice_in_dim(heads, first, share, 0)
        if step:
            ring = [(i, (i + step) % planes) for i in range(planes)]
            piece = lax.ppermute(piece, "tp", ring)
        pieces.append(piece)
    mixed_rows = call(
        project_body,
        struct((share, d), bf16),
        where,
        *pieces,
        out_weight,
        out_gain.reshape(1, d),
        cost=20 * positions * width * d,
        specs=[sm] + [vm] * (planes + 2),
    )
    part = d // 4
    back = back.reshape(slots, d + d // 2)
    routed_rows = call(
        combine_body,
        struct((tokens, d), bf16),
        share8,
        share4,
        back,
        back,
        cost=12 * tokens * slots * d,
        grid=(4,),
        specs=[
            whole(2 * tokens, slots),
            pl.BlockSpec((1, 2 * tokens, slots), lambda i: (i // 2, 0, 0)),
            pl.BlockSpec((slots, part), lambda i: (0, i)),
            pl.BlockSpec((slots, part), lambda i: (0, 4 + i % 2)),
        ],
        out_specs=pl.BlockSpec((tokens, part), lambda i: (0, i)),
        vmem=60,
    )
    return (mixed_rows, routed_rows)


def solution(mesh):
    finer = Mesh(mesh.devices.reshape(8, 4, 2, mesh.shape["tp"]), ("ep_0", "ep_1", "ep_2", "tp"))
    in_specs = (
        P(EP, "tp"),
        P(EP, "tp"),
        P(EP, "tp"),
        P("tp", EP),
        P("tp", EP),
        P("tp", EP),
        P("tp"),
        P(),
        P(),
        P(EP_TP, None),
        P(),
        P(EP_TP, None),
        P(EP_TP),
        P(EP_TP, None),
        P(EP, None, None),
        P(EP, None, None),
        P(EP, None, None),
    )
    out_specs = (P(EP_TP, None), P(EP_TP, None))
    return jax.shard_map(
        shards, mesh=finer, in_specs=in_specs, out_specs=out_specs, check_vma=False
    )
```

```python
import jax
import jax.numpy as jnp
from jax import lax
from jax.experimental import pallas as pl
from jax.experimental.pallas import tpu as pltpu
from jax.sharding import Mesh
from jax.sharding import PartitionSpec as P

EP = ("ep_0", "ep_1", "ep_2")
EP_TP = ("ep_0", "ep_1", "ep_2", "tp")


floor_log = -1e30
norm_eps = 1e-06
f32, bf16, i32 = jnp.float32, jnp.bfloat16, jnp.int32


def iota(shape, dim):
    return lax.broadcasted_iota(i32, shape, dim)


def mm(a, b):
    return lax.dot_general(a, b, (((1,), (0,)), ((), ())), preferred_element_type=f32)


def mm_t(a, b):
    return lax.dot_general(a, b, (((1,), (1,)), ((), ())), preferred_element_type=f32)


def thirds(x):
    hi = x.astype(bf16).astype(f32)
    mid = (x - hi).astype(bf16).astype(f32)
    return hi, mid, (x - hi - mid).astype(bf16).astype(f32)


def halves(x):
    hi = x.astype(bf16)
    return hi, (x - hi.astype(f32)).astype(bf16)


def call(body, out_shape, *args, cost, scratch=(), specs=None, out_specs=None, grid=None, vmem=24):
    extra = {}
    if grid is not None:
        extra = dict(grid=grid, in_specs=specs, out_specs=out_specs)
    elif specs is not None:
        extra = dict(in_specs=specs)
        if out_specs is not None:
            extra["out_specs"] = out_specs
    return pl.pallas_call(
        body,
        out_shape=out_shape,
        scratch_shapes=list(scratch),
        compiler_params=pltpu.CompilerParams(vmem_limit_bytes=vmem << 20),
        cost_estimate=pl.CostEstimate(flops=cost, bytes_accessed=cost // 500, transcendentals=0),
        **extra,
    )(*args)


def struct(shape, dtype):
    return jax.ShapeDtypeStruct(shape, dtype)


def build_body(ids_far, rows_far, gain_far, out, ranks, ids, rows, gain, made, sems, out_sems):
    tokens, d = rows.shape
    half = d // 2
    experts = ranks.shape[0]
    loads = [
        pltpu.make_async_copy(far, near, sems.at[k])
        for k, (far, near) in enumerate(((ids_far, ids), (rows_far, rows), (gain_far, gain)))
    ]
    for load in loads:
        load.start()
    ahead = (iota((tokens, tokens), 0) < iota((tokens, tokens), 1)).astype(f32).astype(bf16)
    expert = iota((experts, tokens), 0)
    loads[0].wait()
    chosen = (ids[0:1, :] == expert) | (ids[1:2, :] == expert)
    count = mm(chosen.astype(f32).astype(bf16), ahead)
    rank = jnp.where(chosen, count, -1.0)
    ranks[...] = rank
    loads[1].wait()
    x = rows[...].astype(f32)
    mean = jnp.mean(x * x, axis=-1, keepdims=True)
    loads[2].wait()
    xn = (x * lax.rsqrt(mean + norm_eps) * gain[...]).astype(bf16)
    steps, block, _ = made.shape
    part = block // 8
    row = iota((part, 8, tokens), 1)
    slot = row.astype(f32)
    late_slot = ((row & 3) + 8).astype(f32)

    def placing(hit):
        return hit.astype(f32).reshape(block, tokens).astype(bf16)

    def store(step):
        return pltpu.make_async_copy(
            made.at[step], out.at[pl.ds(step * block, block), :], out_sems.at[step]
        )

    for step in range(steps):
        held = rank[step * part : (step + 1) * part, None, :]
        made[step, :, :d] = mm(placing(held == slot), xn).astype(bf16)
        late = held == late_slot
        first, last = placing(late & (row < 4)), placing(late & (row >= 4))
        made[step, :, d:] = (mm(first, xn[:, :half]) + mm(last, xn[:, half:])).astype(bf16)
        store(step).start()
    for step in range(steps):
        store(step).wait()


def silu_mul(gate, upper):
    return (gate / (1.0 + jnp.exp(-gate)) * upper).astype(bf16)


def ffn_body(x_far, wg_far, wu_far, wd_far, out, x, wg, wu, wd, made, in_sems, sems):
    d, _ = wg.shape
    half = d // 2
    slots = x.shape[0]
    pieces = (
        (x_far.at[:, pl.ds(d, half)], x.at[:, pl.ds(d, half)]),
        (wg_far.at[pl.ds(0, half), :], wg.at[pl.ds(0, half), :]),
        (wg_far.at[pl.ds(half, half), :], wg.at[pl.ds(half, half), :]),
        (wu_far, wu),
        (x_far.at[:, pl.ds(0, d)], x.at[:, pl.ds(0, d)]),
        (wd_far, wd),
    )
    loads = [
        pltpu.make_async_copy(far, near, in_sems.at[k]) for k, (far, near) in enumerate(pieces)
    ]
    for load in loads:
        load.start()
    pairs = slots // 16

    def crossed(left, right):
        upper = (iota((1, 8, 1), 1) & 4) == 0
        return (
            jnp.where(upper, left, pltpu.roll(right, 4, 1)),
            jnp.where(upper, pltpu.roll(left, 4, 1), right),
        )

    loads[0].wait()
    x4 = x[:, d:].astype(f32).reshape(pairs, 2, 8, half)
    top, bottom = crossed(x4[:, 0], x4[:, 1])
    top = top.reshape(pairs * 8, half).astype(bf16)
    bottom = bottom.reshape(pairs * 8, half).astype(bf16)
    loads[1].wait()
    gate4 = mm(top, wg[:half, :])
    loads[2].wait()
    gate4 += mm(bottom, wg[half:, :])
    loads[3].wait()
    hidden4 = silu_mul(gate4, mm(top, wu[:half, :]) + mm(bottom, wu[half:, :]))
    loads[4].wait()
    x8 = x[:, :d]
    hidden8 = silu_mul(mm(x8, wg[...]), mm(x8, wu[...]))
    loads[5].wait()
    part = made.shape[2]
    stores = []

    def send(step, values):
        made[step] = values.astype(bf16)
        stores.append(
            pltpu.make_async_copy(
                made.at[step], out.at[:, pl.ds(step * part, part)], sems.at[step]
            )
        )
        stores[-1].start()

    early = d // part
    for step in range(early):
        send(step, mm(hidden8, wd[:, step * part : (step + 1) * part]))
    for step in range(half // part):
        cols = slice(step * part, (step + 1) * part)
        far = slice(half + step * part, half + (step + 1) * part)
        left = mm(hidden4, wd[:, cols]).reshape(pairs, 8, part)
        right = mm(hidden4, wd[:, far]).reshape(pairs, 8, part)
        both = jnp.stack(crossed(left, right), axis=1)
        send(early + step, both.reshape(slots, part))
    for store in stores:
        store.wait()


def combine_body(ids, prob, scores, ranks, back, out):
    rank = ranks[...]
    experts, tokens = rank.shape
    s0, s1 = scores[0:1, :], scores[1:2, :]
    top = jnp.maximum(s0, s1)
    e0, e1 = jnp.exp(s0 - top), jnp.exp(s1 - top)
    both = e0 + e1
    w0, w1 = prob[...] * (e0 / both), prob[...] * (e1 / both)
    expert = iota((experts, tokens), 0)
    share = jnp.where(ids[0:1, :] == expert, w0, 0.0) + jnp.where(ids[1:2, :] == expert, w1, 0.0)
    row = iota((experts, 8, tokens), 1)

    def placed(hit):
        at = jnp.where(hit, share[:, None, :], 0.0).reshape(experts * 8, tokens)
        return at.T.astype(bf16)

    early = placed(rank[:, None, :] == row.astype(f32))
    hit = rank[:, None, :] == ((row & 3) + 8).astype(f32)
    half = out.shape[1] // 2
    late = back[:, 2 * half :]
    for h in range(2):
        cols = slice(h * half, (h + 1) * half)
        extra = mm(placed(hit & ((row >> 2) == h)), late)
        out[:, cols] = (mm(early, back[:, cols]) + extra).astype(bf16)


def running_keep(forget, boosts):
    x = forget[...]
    keep = boosts[...] - (jnp.maximum(-x, 0.0) + jnp.log1p(jnp.exp(-jnp.abs(x))))
    length = keep.shape[1]
    pieces = jnp.concatenate([*thirds(keep), jnp.zeros((5, length), f32)], axis=0).astype(bf16)
    upto = (iota((length, length), 0) <= iota((length, length), 1)).astype(f32).astype(bf16)
    return jnp.sum(mm(pieces, upto), axis=0, keepdims=True)


def side_rows(normer, total, peak):
    width = normer.shape[1]
    hi = normer.astype(bf16).astype(f32)
    lane = iota((1, width), 1)
    info = jnp.zeros((1, width), f32)
    for at, piece in enumerate((*thirds(total), *thirds(peak))):
        info = jnp.where(lane == at, piece, info)
    return jnp.concatenate([hi, normer - hi, info, jnp.zeros((5, width), f32)], axis=0)


def read_side(side):
    normer = side[0:1, :] + side[1:2, :]
    info = side[2:3, :]
    total = info[:, 0:1] + info[:, 1:2] + info[:, 2:3]
    peak = info[:, 3:4] + info[:, 4:5] + info[:, 5:6]
    return normer, total, peak


def summary_body(keys, values, gates, forget, boosts, out, rest):
    b = running_keep(forget, boosts)
    length = b.shape[1]
    width = keys.shape[1]
    last = b[:, length - 1 : length]
    gap = last - b + gates[...]
    peak = jnp.max(gap, axis=1, keepdims=True)
    spread = jnp.exp(gap - peak) * (width**-0.5)
    k = keys[...]
    scaled = (values[...].astype(f32).T * spread).astype(bf16)
    half = width // 2
    memory = mm(scaled, k).astype(bf16)
    out[:half, :] = memory[:half]
    rest[...] = memory[half:]
    hi, lo = halves(spread)
    two = jnp.concatenate([hi.astype(f32), lo.astype(f32), jnp.zeros((6, length), f32)], axis=0)
    normer = jnp.sum(mm(two.astype(bf16), k), axis=0, keepdims=True)
    out[half:, :] = side_rows(normer, last, peak).astype(bf16)


def weighted(pieces, logs, floor):
    stabil = floor
    for level in logs:
        stabil = jnp.maximum(stabil, level)
    memory, normer = None, None
    for (piece, n), level in zip(pieces, logs):
        factor = jnp.exp(level - stabil)
        memory = factor * piece if memory is None else memory + factor * piece
        normer = factor * n if normer is None else normer + factor * n
    return memory, normer, stabil


def before(mine, totals, peaks):
    logs, kept = [], []
    floor = jnp.full((1, 1), floor_log, f32)
    for j in range(len(totals)):
        level = peaks[j]
        for l in range(j + 1, len(totals)):
            level = level + jnp.where(l < mine, totals[l], 0.0)
        kept.append(j < mine)
        logs.append(jnp.where(j < mine, level, floor))
    return logs, kept


def masked(kept, pieces):
    return [(jnp.where(k, c, 0.0), jnp.where(k, n, 0.0)) for k, (c, n) in zip(kept, pieces)]


def plane_body(where, got, more, out, own, small, whole_memory):
    mine = where[1]
    width = got.shape[2]
    half = width // 2
    count = got.shape[0]
    pieces, totals, peaks = [], [], []
    for j in range(count):
        normer, total, peak = read_side(got[j, half:, :].astype(f32))
        memory = jnp.concatenate([got[j, :half, :], more[j]], axis=0).astype(f32)
        pieces.append((memory, normer))
        totals.append(total)
        peaks.append(peak)
    logs = []
    for j in range(count):
        level = peaks[j]
        for l in range(j + 1, count):
            level = level + totals[l]
        logs.append(level)
    memory, normer, stabil = weighted(pieces, logs, logs[0])
    everything = totals[0]
    for total in totals[1:]:
        everything = everything + total
    whole_memory[...] = memory
    part = width // count
    out[:part, :] = whole_memory[pl.ds(pl.multiple_of(mine * part, 8), part), :].astype(bf16)
    out[part:, :] = side_rows(normer, everything, stabil).astype(bf16)
    logs, kept = before(mine, totals, peaks)
    memory, normer, stabil = weighted(
        masked(kept, pieces), logs, jnp.full((1, 1), floor_log, f32)
    )
    own[...] = memory
    passed = jnp.zeros((1, 1), f32)
    for l in range(count):
        passed = passed + jnp.where(l < mine, totals[l], 0.0)
    small[0:1, :] = normer
    small[1:2, :] = jnp.broadcast_to(stabil, (1, width))
    small[2:3, :] = jnp.broadcast_to(passed, (1, width))
    small[3:8, :] = jnp.zeros((5, width), f32)


def line_body(where, *refs):
    got, (out, small) = refs[:-2], refs[-2:]
    mine = where[0]
    part, width = out.shape
    floor = jnp.full((1, 1), floor_log, f32)
    passed = jnp.zeros((1, 1), f32)
    pieces, logs, kept = [], [], []
    for step, piece in enumerate(got):
        normer, total, peak = read_side(piece[part:, :].astype(f32))
        near = step < mine
        pieces.append((piece[:part, :].astype(f32), normer))
        logs.append(jnp.where(near, peak + passed, floor))
        kept.append(near)
        passed = passed + jnp.where(near, total, 0.0)
    memory, normer, stabil = weighted(masked(kept, pieces), logs, floor)
    out[...] = memory.astype(bf16)
    small[0:1, :] = normer
    small[1:2, :] = jnp.broadcast_to(stabil, (1, width))
    small[2:8, :] = jnp.zeros((6, width), f32)


def cell_body(query, keys, values, gates, forget, boosts, state, line, own, near, scale, out):
    b = running_keep(forget, boosts)
    length = b.shape[1]
    width = keys.shape[1]
    b_col = jnp.broadcast_to(b, (128, length)).T
    far_log = near[2:3, 0:1] + line[1:2, 0:1]
    near_log = near[1:2, 0:1]
    stabil = jnp.maximum(far_log, near_log)
    far, close = jnp.exp(far_log - stabil), jnp.exp(near_log - stabil)
    normer = far * line[0:1, :] + close * near[0:1, :]
    memory = (far * state[...].astype(f32) + close * own[...]).astype(bf16)
    source = gates[...] - b
    block = 128
    for start in range(0, length, block):
        upto = start + block
        rows = slice(start, upto)
        q = query[rows, :]
        bt = b_col[rows, 0:1]
        decay = bt + source[:, :upto]
        seen = iota((block, upto), 1) <= iota((block, upto), 0) + start
        decay = jnp.where(seen, decay, -jnp.inf)
        carried = bt + stabil
        peak = jnp.maximum(carried, jnp.max(decay, axis=1, keepdims=True))
        across = jnp.exp(carried - peak)
        scores = mm_t(q, keys[:upto, :]) * (width**-0.5) * jnp.exp(decay - peak)
        den = jnp.sum(scores, axis=1, keepdims=True) + across * jnp.sum(
            q.astype(f32) * normer, axis=1, keepdims=True
        )
        num = mm(scores.astype(bf16), values[:upto, :]) + across * mm_t(q, memory)
        cell = num / jnp.maximum(jnp.abs(den), jnp.exp(-peak))
        out[rows, :] = (cell * scale[...]).astype(bf16)


def project_body(where, *refs):
    heads, (weight, gain, out) = refs[:-3], refs[-3:]
    count = len(heads)
    width = heads[0].shape[-1]
    total = None
    for step, head in enumerate(heads):
        source = lax.rem(where[2] + count - step, count)
        rows = weight[pl.ds(pl.multiple_of(source * width, width), width), :]
        product = mm(head[...], rows)
        total = product if total is None else total + product
    mean = jnp.mean(total * total, axis=-1, keepdims=True)
    out[...] = (total * lax.rsqrt(mean + norm_eps) * gain[...]).astype(bf16)


def exchanged(array, axes):
    return lax.all_to_all(array, axes, split_axis=0, concat_axis=0, tiled=True)


def after(array, *earlier):
    return lax.optimization_barrier((array, *earlier))[0]


def shards(
    query,
    keys,
    values,
    in_gates,
    forget,
    boosts,
    head_scale,
    out_weight,
    out_gain,
    rows,
    row_gain,
    ids,
    prob,
    scores,
    w_gate,
    w_up,
    w_down,
):
    devices = lax.axis_size(EP)
    positions, width = query.shape
    tokens, d = rows.shape
    hidden = w_gate.shape[2]
    slots = devices * 8
    line, plane = lax.axis_size("ep_0"), lax.axis_size(("ep_1", "ep_2"))
    planes = lax.axis_size("tp")
    ids_t = ids.T
    vm = pl.BlockSpec(memory_space=pltpu.VMEM)
    sm = pl.BlockSpec(memory_space=pltpu.SMEM)
    far_away = pl.BlockSpec(memory_space=pltpu.HBM)
    where = jnp.stack(
        [lax.axis_index("ep_0"), lax.axis_index(("ep_1", "ep_2")), lax.axis_index("tp")]
    ).astype(i32)

    out, ranks = call(
        build_body,
        (struct((slots, d + d // 2), bf16), struct((devices, tokens), f32)),
        ids_t,
        rows,
        row_gain.reshape(1, d),
        cost=4 * slots * tokens * d,
        specs=[far_away] * 3,
        out_specs=(far_away, vm),
        scratch=(
            pltpu.VMEM((2, tokens), i32),
            pltpu.VMEM((tokens, d), bf16),
            pltpu.VMEM((1, d), f32),
            pltpu.VMEM((4, slots // 4, d + d // 2), bf16),
            pltpu.SemaphoreType.DMA((3,)),
            pltpu.SemaphoreType.DMA((4,)),
        ),
        vmem=60,
    )
    got = exchanged(out.reshape(devices, 8, d + d // 2), EP)
    send, rest = call(
        summary_body,
        (struct((width // 2 + 8, width), bf16), struct((width // 2, width), bf16)),
        after(keys, out),
        values,
        in_gates,
        forget,
        boosts,
        cost=2 * positions * width * width * 4,
    )
    states = lax.all_gather(send, ("ep_1", "ep_2"))
    more = lax.all_gather(after(rest, states), ("ep_1", "ep_2"))
    send, own, near = call(
        plane_body,
        (
            struct((width // plane + 8, width), bf16),
            struct((width, width), f32),
            struct((8, width), f32),
        ),
        where,
        states,
        more,
        cost=4 * plane * width * width * 100,
        scratch=(pltpu.VMEM((width, width), f32),),
        specs=[sm, vm, vm],
    )
    states = [
        lax.ppermute(send, "ep_0", [(i, i + step) for i in range(line - step)])
        for step in range(1, line)
    ]
    send, far = call(
        line_body,
        (struct((width // plane, width), bf16), struct((8, width), f32)),
        where,
        *states,
        cost=4 * width * width * 100,
        specs=[sm] + [vm] * (line - 1),
    )
    answers = call(
        ffn_body,
        struct((slots, d + d // 2), bf16),
        after(got, send).reshape(slots, d + d // 2),
        w_gate[0],
        w_up[0],
        w_down[0],
        cost=12 * slots * d * hidden,
        specs=[far_away] * 4,
        out_specs=far_away,
        scratch=(
            pltpu.VMEM((slots, d + d // 2), bf16),
            pltpu.VMEM((d, hidden), bf16),
            pltpu.VMEM((d, hidden), bf16),
            pltpu.VMEM((hidden, d), bf16),
            pltpu.VMEM((6, slots, d // 4), bf16),
            pltpu.SemaphoreType.DMA((6,)),
            pltpu.SemaphoreType.DMA((6,)),
        ),
        vmem=60,
    )
    back = exchanged(answers.reshape(devices, 8, d + d // 2), EP)
    state = lax.all_gather(send, ("ep_1", "ep_2"), tiled=True)
    heads = call(
        cell_body,
        struct((positions, width), bf16),
        query,
        keys,
        values,
        in_gates,
        forget,
        boosts,
        state,
        far,
        own,
        near,
        head_scale.reshape(1, width),
        cost=2 * positions * positions * width * 40,
    )
    share = positions // planes
    me = where[2]
    pieces = []
    for step in range(planes):
        first = lax.rem(me + step, planes) * share
        piece = lax.dynamic_slice_in_dim(heads, first, share, 0)
        if step:
            ring = [(i, (i + step) % planes) for i in range(planes)]
            piece = lax.ppermute(piece, "tp", ring)
        pieces.append(piece)
    mixed_rows = call(
        project_body,
        struct((share, d), bf16),
        where,
        *pieces,
        out_weight,
        out_gain.reshape(1, d),
        cost=20 * positions * width * d,
        specs=[sm] + [vm] * (planes + 2),
    )
    routed_rows = call(
        combine_body,
        struct((tokens, d), bf16),
        ids_t,
        prob.reshape(1, tokens),
        scores.T,
        ranks,
        back.reshape(slots, d + d // 2),
        cost=12 * tokens * slots * d,
        vmem=16,
    )
    return (mixed_rows, routed_rows)


def solution(mesh):
    finer = Mesh(mesh.devices.reshape(8, 4, 2, mesh.shape["tp"]), ("ep_0", "ep_1", "ep_2", "tp"))
    in_specs = (
        P(EP, "tp"),
        P(EP, "tp"),
        P(EP, "tp"),
        P("tp", EP),
        P("tp", EP),
        P("tp", EP),
        P("tp"),
        P(),
        P(),
        P(EP_TP, None),
        P(),
        P(EP_TP, None),
        P(EP_TP),
        P(EP_TP, None),
        P(EP, None, None),
        P(EP, None, None),
        P(EP, None, None),
    )
    out_specs = (P(EP_TP, None), P(EP_TP, None))
    return jax.shard_map(
        shards, mesh=finer, in_specs=in_specs, out_specs=out_specs, check_vma=False
    )
```

```python
import jax
import jax.numpy as jnp
from jax import lax
from jax.experimental import pallas as pl
from jax.experimental.pallas import tpu as pltpu
from jax.sharding import Mesh
from jax.sharding import PartitionSpec as P

EP = ("ep_0", "ep_1", "ep_2")
EP_TP = ("ep_0", "ep_1", "ep_2", "tp")


floor_log = -1e30
norm_eps = 1e-06
f32, bf16, i32 = jnp.float32, jnp.bfloat16, jnp.int32


def iota(shape, dim):
    return lax.broadcasted_iota(i32, shape, dim)


def mm(a, b):
    return lax.dot_general(a, b, (((1,), (0,)), ((), ())), preferred_element_type=f32)


def mm_t(a, b):
    return lax.dot_general(a, b, (((1,), (1,)), ((), ())), preferred_element_type=f32)


def thirds(x):
    hi = x.astype(bf16).astype(f32)
    mid = (x - hi).astype(bf16).astype(f32)
    return hi, mid, (x - hi - mid).astype(bf16).astype(f32)


def halves(x):
    hi = x.astype(bf16)
    return hi, (x - hi.astype(f32)).astype(bf16)


def call(body, out_shape, *args, cost, scratch=(), specs=None, out_specs=None, grid=None, vmem=24):
    extra = {}
    if grid is not None:
        extra = dict(grid=grid, in_specs=specs, out_specs=out_specs)
    elif specs is not None:
        extra = dict(in_specs=specs)
        if out_specs is not None:
            extra["out_specs"] = out_specs
    return pl.pallas_call(
        body,
        out_shape=out_shape,
        scratch_shapes=list(scratch),
        compiler_params=pltpu.CompilerParams(vmem_limit_bytes=vmem << 20),
        cost_estimate=pl.CostEstimate(flops=cost, bytes_accessed=cost // 500, transcendentals=0),
        **extra,
    )(*args)


def struct(shape, dtype):
    return jax.ShapeDtypeStruct(shape, dtype)


def build_body(
    ids_far, rows_far, gain_far, out, ranks, ids, rows, gain, places, made, sems, out_sems
):
    tokens, d = rows.shape
    half = d // 2
    experts = ranks.shape[0]
    loads = [
        pltpu.make_async_copy(far, near, sems.at[k])
        for k, (far, near) in enumerate(((ids_far, ids), (rows_far, rows), (gain_far, gain)))
    ]
    for load in loads:
        load.start()
    ahead = (iota((tokens, tokens), 0) < iota((tokens, tokens), 1)).astype(f32).astype(bf16)
    expert = iota((experts, tokens), 0)
    loads[0].wait()
    chosen = (ids[0:1, :] == expert) | (ids[1:2, :] == expert)
    count = mm(chosen.astype(f32).astype(bf16), ahead)
    rank = jnp.where(chosen, count, -1.0)
    ranks[...] = rank
    _, slots, part = made.shape
    row = iota((experts, 8, tokens), 1)
    held = rank[:, None, :]

    def placing(hit):
        return hit.astype(f32).reshape(slots, tokens).astype(bf16)

    late = held == ((row & 3) + 8).astype(f32)
    places[0] = placing(held == row.astype(f32))
    places[1] = placing(late & (row < 4))
    places[2] = placing(late & (row >= 4))
    loads[1].wait()
    x = rows[...].astype(f32)
    mean = jnp.mean(x * x, axis=-1, keepdims=True)
    loads[2].wait()
    xn = (x * lax.rsqrt(mean + norm_eps) * gain[...]).astype(bf16)
    stores = []

    def send(step, values):
        made[step] = values.astype(bf16)
        stores.append(
            pltpu.make_async_copy(
                made.at[step], out.at[:, pl.ds(step * part, part)], out_sems.at[step]
            )
        )
        stores[-1].start()

    early = d // part
    for step in range(early):
        send(step, mm(places[0], xn[:, step * part : (step + 1) * part]))
    for step in range(half // part):
        left = xn[:, step * part : (step + 1) * part]
        right = xn[:, half + step * part : half + (step + 1) * part]
        send(early + step, mm(places[1], left) + mm(places[2], right))
    for store in stores:
        store.wait()


def silu_mul(gate, upper):
    return (gate / (1.0 + jnp.exp(-gate)) * upper).astype(bf16)


def ffn_body(x_far, wg, wu_far, wd_far, out, x, wu, wd, made, in_sems, sems):
    d, _ = wg.shape
    half = d // 2
    slots = x.shape[0]
    pieces = (
        (x_far.at[:, pl.ds(d, half)], x.at[:, pl.ds(d, half)]),
        (x_far.at[:, pl.ds(0, d)], x.at[:, pl.ds(0, d)]),
        (wu_far, wu),
        (wd_far, wd),
    )
    loads = [
        pltpu.make_async_copy(far, near, in_sems.at[k]) for k, (far, near) in enumerate(pieces)
    ]
    for load in loads:
        load.start()
    pairs = slots // 16

    def crossed(left, right):
        upper = (iota((1, 8, 1), 1) & 4) == 0
        return (
            jnp.where(upper, left, pltpu.roll(right, 4, 1)),
            jnp.where(upper, pltpu.roll(left, 4, 1), right),
        )

    loads[0].wait()
    x4 = x[:, d:].astype(f32).reshape(pairs, 2, 8, half)
    top, bottom = crossed(x4[:, 0], x4[:, 1])
    top = top.reshape(pairs * 8, half).astype(bf16)
    bottom = bottom.reshape(pairs * 8, half).astype(bf16)
    gate4 = mm(top, wg[:half, :]) + mm(bottom, wg[half:, :])
    loads[1].wait()
    x8 = x[:, :d]
    gate8 = mm(x8, wg[...])
    loads[2].wait()
    hidden4 = silu_mul(gate4, mm(top, wu[:half, :]) + mm(bottom, wu[half:, :]))
    hidden8 = silu_mul(gate8, mm(x8, wu[...]))
    loads[3].wait()
    part = made.shape[2]
    stores = []

    def send(step, values):
        made[step] = values.astype(bf16)
        stores.append(
            pltpu.make_async_copy(
                made.at[step], out.at[:, pl.ds(step * part, part)], sems.at[step]
            )
        )
        stores[-1].start()

    early = d // part
    for step in range(early):
        send(step, mm(hidden8, wd[:, step * part : (step + 1) * part]))
    for step in range(half // part):
        cols = slice(step * part, (step + 1) * part)
        far = slice(half + step * part, half + (step + 1) * part)
        left = mm(hidden4, wd[:, cols]).reshape(pairs, 8, part)
        right = mm(hidden4, wd[:, far]).reshape(pairs, 8, part)
        both = jnp.stack(crossed(left, right), axis=1)
        send(early + step, both.reshape(slots, part))
    for store in stores:
        store.wait()


def combine_body(ids, prob, scores, ranks, back, out):
    rank = ranks[...]
    experts, tokens = rank.shape
    s0, s1 = scores[0:1, :], scores[1:2, :]
    top = jnp.maximum(s0, s1)
    e0, e1 = jnp.exp(s0 - top), jnp.exp(s1 - top)
    both = e0 + e1
    w0, w1 = prob[...] * (e0 / both), prob[...] * (e1 / both)
    expert = iota((experts, tokens), 0)
    share = jnp.where(ids[0:1, :] == expert, w0, 0.0) + jnp.where(ids[1:2, :] == expert, w1, 0.0)
    row = iota((experts, 8, tokens), 1)

    def placed(hit):
        at = jnp.where(hit, share[:, None, :], 0.0).reshape(experts * 8, tokens)
        return at.T.astype(bf16)

    early = placed(rank[:, None, :] == row.astype(f32))
    hit = rank[:, None, :] == ((row & 3) + 8).astype(f32)
    half = out.shape[1] // 2
    late = back[:, 2 * half :]
    for h in range(2):
        cols = slice(h * half, (h + 1) * half)
        extra = mm(placed(hit & ((row >> 2) == h)), late)
        out[:, cols] = (mm(early, back[:, cols]) + extra).astype(bf16)


def running_keep(forget, boosts):
    x = forget[...]
    keep = boosts[...] - (jnp.maximum(-x, 0.0) + jnp.log1p(jnp.exp(-jnp.abs(x))))
    length = keep.shape[1]
    pieces = jnp.concatenate([*thirds(keep), jnp.zeros((5, length), f32)], axis=0).astype(bf16)
    upto = (iota((length, length), 0) <= iota((length, length), 1)).astype(f32).astype(bf16)
    return jnp.sum(mm(pieces, upto), axis=0, keepdims=True)


def side_rows(normer, total, peak):
    width = normer.shape[1]
    hi = normer.astype(bf16).astype(f32)
    lane = iota((1, width), 1)
    info = jnp.zeros((1, width), f32)
    for at, piece in enumerate((*thirds(total), *thirds(peak))):
        info = jnp.where(lane == at, piece, info)
    return jnp.concatenate([hi, normer - hi, info, jnp.zeros((5, width), f32)], axis=0)


def read_side(side):
    normer = side[0:1, :] + side[1:2, :]
    info = side[2:3, :]
    total = info[:, 0:1] + info[:, 1:2] + info[:, 2:3]
    peak = info[:, 3:4] + info[:, 4:5] + info[:, 5:6]
    return normer, total, peak


def summary_body(keys, values, gates, forget, boosts, out, rest):
    b = running_keep(forget, boosts)
    length = b.shape[1]
    width = keys.shape[1]
    last = b[:, length - 1 : length]
    gap = last - b + gates[...]
    peak = jnp.max(gap, axis=1, keepdims=True)
    spread = jnp.exp(gap - peak) * (width**-0.5)
    k = keys[...]
    scaled = (values[...].astype(f32).T * spread).astype(bf16)
    half = width // 2
    memory = mm(scaled, k).astype(bf16)
    out[:half, :] = memory[:half]
    rest[...] = memory[half:]
    hi, lo = halves(spread)
    two = jnp.concatenate([hi.astype(f32), lo.astype(f32), jnp.zeros((6, length), f32)], axis=0)
    normer = jnp.sum(mm(two.astype(bf16), k), axis=0, keepdims=True)
    out[half:, :] = side_rows(normer, last, peak).astype(bf16)


def weighted(pieces, logs, floor):
    stabil = floor
    for level in logs:
        stabil = jnp.maximum(stabil, level)
    memory, normer = None, None
    for (piece, n), level in zip(pieces, logs):
        factor = jnp.exp(level - stabil)
        memory = factor * piece if memory is None else memory + factor * piece
        normer = factor * n if normer is None else normer + factor * n
    return memory, normer, stabil


def before(mine, totals, peaks):
    logs, kept = [], []
    floor = jnp.full((1, 1), floor_log, f32)
    for j in range(len(totals)):
        level = peaks[j]
        for l in range(j + 1, len(totals)):
            level = level + jnp.where(l < mine, totals[l], 0.0)
        kept.append(j < mine)
        logs.append(jnp.where(j < mine, level, floor))
    return logs, kept


def masked(kept, pieces):
    return [(jnp.where(k, c, 0.0), jnp.where(k, n, 0.0)) for k, (c, n) in zip(kept, pieces)]


def plane_body(where, got, more, out, own, small, whole_memory):
    mine = where[1]
    width = got.shape[2]
    half = width // 2
    count = got.shape[0]
    pieces, totals, peaks = [], [], []
    for j in range(count):
        normer, total, peak = read_side(got[j, half:, :].astype(f32))
        memory = jnp.concatenate([got[j, :half, :], more[j]], axis=0).astype(f32)
        pieces.append((memory, normer))
        totals.append(total)
        peaks.append(peak)
    logs = []
    for j in range(count):
        level = peaks[j]
        for l in range(j + 1, count):
            level = level + totals[l]
        logs.append(level)
    memory, normer, stabil = weighted(pieces, logs, logs[0])
    everything = totals[0]
    for total in totals[1:]:
        everything = everything + total
    whole_memory[...] = memory
    part = width // count
    out[:part, :] = whole_memory[pl.ds(pl.multiple_of(mine * part, 8), part), :].astype(bf16)
    out[part:, :] = side_rows(normer, everything, stabil).astype(bf16)
    logs, kept = before(mine, totals, peaks)
    memory, normer, stabil = weighted(
        masked(kept, pieces), logs, jnp.full((1, 1), floor_log, f32)
    )
    own[...] = memory
    passed = jnp.zeros((1, 1), f32)
    for l in range(count):
        passed = passed + jnp.where(l < mine, totals[l], 0.0)
    small[0:1, :] = normer
    small[1:2, :] = jnp.broadcast_to(stabil, (1, width))
    small[2:3, :] = jnp.broadcast_to(passed, (1, width))
    small[3:8, :] = jnp.zeros((5, width), f32)


def line_body(where, *refs):
    got, (out, small) = refs[:-2], refs[-2:]
    mine = where[0]
    part, width = out.shape
    floor = jnp.full((1, 1), floor_log, f32)
    passed = jnp.zeros((1, 1), f32)
    pieces, logs, kept = [], [], []
    for step, piece in enumerate(got):
        normer, total, peak = read_side(piece[part:, :].astype(f32))
        near = step < mine
        pieces.append((piece[:part, :].astype(f32), normer))
        logs.append(jnp.where(near, peak + passed, floor))
        kept.append(near)
        passed = passed + jnp.where(near, total, 0.0)
    memory, normer, stabil = weighted(masked(kept, pieces), logs, floor)
    out[...] = memory.astype(bf16)
    small[0:1, :] = normer
    small[1:2, :] = jnp.broadcast_to(stabil, (1, width))
    small[2:8, :] = jnp.zeros((6, width), f32)


def cell_body(query, keys, values, gates, forget, boosts, state, line, own, near, scale, out):
    b = running_keep(forget, boosts)
    length = b.shape[1]
    width = keys.shape[1]
    b_col = jnp.broadcast_to(b, (128, length)).T
    far_log = near[2:3, 0:1] + line[1:2, 0:1]
    near_log = near[1:2, 0:1]
    stabil = jnp.maximum(far_log, near_log)
    far, close = jnp.exp(far_log - stabil), jnp.exp(near_log - stabil)
    normer = far * line[0:1, :] + close * near[0:1, :]
    memory = (far * state[...].astype(f32) + close * own[...]).astype(bf16)
    source = gates[...] - b
    block = 128
    for start in range(0, length, block):
        upto = start + block
        rows = slice(start, upto)
        q = query[rows, :]
        bt = b_col[rows, 0:1]
        decay = bt + source[:, :upto]
        seen = iota((block, upto), 1) <= iota((block, upto), 0) + start
        decay = jnp.where(seen, decay, -jnp.inf)
        carried = bt + stabil
        peak = jnp.maximum(carried, jnp.max(decay, axis=1, keepdims=True))
        across = jnp.exp(carried - peak)
        scores = mm_t(q, keys[:upto, :]) * (width**-0.5) * jnp.exp(decay - peak)
        den = jnp.sum(scores, axis=1, keepdims=True) + across * jnp.sum(
            q.astype(f32) * normer, axis=1, keepdims=True
        )
        num = mm(scores.astype(bf16), values[:upto, :]) + across * mm_t(q, memory)
        cell = num / jnp.maximum(jnp.abs(den), jnp.exp(-peak))
        out[rows, :] = (cell * scale[...]).astype(bf16)


def project_body(where, *refs):
    heads, (weight, gain, out) = refs[:-3], refs[-3:]
    count = len(heads)
    width = heads[0].shape[-1]
    total = None
    for step, head in enumerate(heads):
        source = lax.rem(where[2] + count - step, count)
        rows = weight[pl.ds(pl.multiple_of(source * width, width), width), :]
        product = mm(head[...], rows)
        total = product if total is None else total + product
    mean = jnp.mean(total * total, axis=-1, keepdims=True)
    out[...] = (total * lax.rsqrt(mean + norm_eps) * gain[...]).astype(bf16)


def exchanged(array, axes):
    return lax.all_to_all(array, axes, split_axis=0, concat_axis=0, tiled=True)


def after(array, *earlier):
    return lax.optimization_barrier((array, *earlier))[0]


def shards(
    query,
    keys,
    values,
    in_gates,
    forget,
    boosts,
    head_scale,
    out_weight,
    out_gain,
    rows,
    row_gain,
    ids,
    prob,
    scores,
    w_gate,
    w_up,
    w_down,
):
    devices = lax.axis_size(EP)
    positions, width = query.shape
    tokens, d = rows.shape
    hidden = w_gate.shape[2]
    slots = devices * 8
    line, plane = lax.axis_size("ep_0"), lax.axis_size(("ep_1", "ep_2"))
    planes = lax.axis_size("tp")
    ids_t = ids.T
    vm = pl.BlockSpec(memory_space=pltpu.VMEM)
    sm = pl.BlockSpec(memory_space=pltpu.SMEM)
    far_away = pl.BlockSpec(memory_space=pltpu.HBM)
    where = jnp.stack(
        [lax.axis_index("ep_0"), lax.axis_index(("ep_1", "ep_2")), lax.axis_index("tp")]
    ).astype(i32)

    out, ranks = call(
        build_body,
        (struct((slots, d + d // 2), bf16), struct((devices, tokens), f32)),
        ids_t,
        rows,
        row_gain.reshape(1, d),
        cost=4 * slots * tokens * d,
        specs=[far_away] * 3,
        out_specs=(far_away, vm),
        scratch=(
            pltpu.VMEM((2, tokens), i32),
            pltpu.VMEM((tokens, d), bf16),
            pltpu.VMEM((1, d), f32),
            pltpu.VMEM((3, slots, tokens), bf16),
            pltpu.VMEM((6, slots, d // 4), bf16),
            pltpu.SemaphoreType.DMA((3,)),
            pltpu.SemaphoreType.DMA((6,)),
        ),
        vmem=60,
    )
    got = exchanged(out.reshape(devices, 8, d + d // 2), EP)
    send, rest = call(
        summary_body,
        (struct((width // 2 + 8, width), bf16), struct((width // 2, width), bf16)),
        after(keys, out),
        values,
        in_gates,
        forget,
        boosts,
        cost=2 * positions * width * width * 4,
    )
    states = lax.all_gather(send, ("ep_1", "ep_2"))
    more = lax.all_gather(after(rest, states), ("ep_1", "ep_2"))
    send, own, near = call(
        plane_body,
        (
            struct((width // plane + 8, width), bf16),
            struct((width, width), f32),
            struct((8, width), f32),
        ),
        where,
        states,
        more,
        cost=4 * plane * width * width * 100,
        scratch=(pltpu.VMEM((width, width), f32),),
        specs=[sm, vm, vm],
    )
    states = [
        lax.ppermute(send, "ep_0", [(i, i + step) for i in range(line - step)])
        for step in range(1, line)
    ]
    send, far = call(
        line_body,
        (struct((width // plane, width), bf16), struct((8, width), f32)),
        where,
        *states,
        cost=4 * width * width * 100,
        specs=[sm] + [vm] * (line - 1),
    )
    answers = call(
        ffn_body,
        struct((slots, d + d // 2), bf16),
        after(got, send).reshape(slots, d + d // 2),
        w_gate[0],
        w_up[0],
        w_down[0],
        cost=12 * slots * d * hidden,
        specs=[far_away, vm, far_away, far_away],
        out_specs=far_away,
        scratch=(
            pltpu.VMEM((slots, d + d // 2), bf16),
            pltpu.VMEM((d, hidden), bf16),
            pltpu.VMEM((hidden, d), bf16),
            pltpu.VMEM((6, slots, d // 4), bf16),
            pltpu.SemaphoreType.DMA((4,)),
            pltpu.SemaphoreType.DMA((6,)),
        ),
        vmem=50,
    )
    back = exchanged(answers.reshape(devices, 8, d + d // 2), EP)
    state = lax.all_gather(send, ("ep_1", "ep_2"), tiled=True)
    heads = call(
        cell_body,
        struct((positions, width), bf16),
        query,
        keys,
        values,
        in_gates,
        forget,
        boosts,
        state,
        far,
        own,
        near,
        head_scale.reshape(1, width),
        cost=2 * positions * positions * width * 40,
    )
    share = positions // planes
    me = where[2]
    pieces = []
    for step in range(planes):
        first = lax.rem(me + step, planes) * share
        piece = lax.dynamic_slice_in_dim(heads, first, share, 0)
        if step:
            ring = [(i, (i + step) % planes) for i in range(planes)]
            piece = lax.ppermute(piece, "tp", ring)
        pieces.append(piece)
    mixed_rows = call(
        project_body,
        struct((share, d), bf16),
        where,
        *pieces,
        out_weight,
        out_gain.reshape(1, d),
        cost=20 * positions * width * d,
        specs=[sm] + [vm] * (planes + 2),
    )
    routed_rows = call(
        combine_body,
        struct((tokens, d), bf16),
        ids_t,
        prob.reshape(1, tokens),
        scores.T,
        ranks,
        back.reshape(slots, d + d // 2),
        cost=12 * tokens * slots * d,
        vmem=16,
    )
    return (mixed_rows, routed_rows)


def solution(mesh):
    finer = Mesh(mesh.devices.reshape(8, 4, 2, mesh.shape["tp"]), ("ep_0", "ep_1", "ep_2", "tp"))
    in_specs = (
        P(EP, "tp"),
        P(EP, "tp"),
        P(EP, "tp"),
        P("tp", EP),
        P("tp", EP),
        P("tp", EP),
        P("tp"),
        P(),
        P(),
        P(EP_TP, None),
        P(),
        P(EP_TP, None),
        P(EP_TP),
        P(EP_TP, None),
        P(EP, None, None),
        P(EP, None, None),
        P(EP, None, None),
    )
    out_specs = (P(EP_TP, None), P(EP_TP, None))
    return jax.shard_map(
        shards, mesh=finer, in_specs=in_specs, out_specs=out_specs, check_vma=False
    )
```

```python
import jax
import jax.numpy as jnp
from jax import lax
from jax.experimental import pallas as pl
from jax.experimental.pallas import tpu as pltpu
from jax.sharding import Mesh
from jax.sharding import PartitionSpec as P

EP = ("ep_0", "ep_1", "ep_2")
EP_TP = ("ep_0", "ep_1", "ep_2", "tp")


floor_log = -1e30
norm_eps = 1e-06
f32, bf16, i32 = jnp.float32, jnp.bfloat16, jnp.int32


def iota(shape, dim):
    return lax.broadcasted_iota(i32, shape, dim)


def mm(a, b):
    return lax.dot_general(a, b, (((1,), (0,)), ((), ())), preferred_element_type=f32)


def mm_t(a, b):
    return lax.dot_general(a, b, (((1,), (1,)), ((), ())), preferred_element_type=f32)


def thirds(x):
    hi = x.astype(bf16).astype(f32)
    mid = (x - hi).astype(bf16).astype(f32)
    return hi, mid, (x - hi - mid).astype(bf16).astype(f32)


def halves(x):
    hi = x.astype(bf16)
    return hi, (x - hi.astype(f32)).astype(bf16)


def call(body, out_shape, *args, cost, scratch=(), specs=None, out_specs=None, grid=None, vmem=24):
    extra = {}
    if grid is not None:
        extra = dict(grid=grid, in_specs=specs, out_specs=out_specs)
    elif specs is not None:
        extra = dict(in_specs=specs)
        if out_specs is not None:
            extra["out_specs"] = out_specs
    return pl.pallas_call(
        body,
        out_shape=out_shape,
        scratch_shapes=list(scratch),
        compiler_params=pltpu.CompilerParams(vmem_limit_bytes=vmem << 20),
        cost_estimate=pl.CostEstimate(flops=cost, bytes_accessed=cost // 500, transcendentals=0),
        **extra,
    )(*args)


def struct(shape, dtype):
    return jax.ShapeDtypeStruct(shape, dtype)


def build_body(
    ids_far, rows_far, gain_far, out, ranks, ids, rows, gain, places, made, sems, out_sems
):
    tokens, d = rows.shape
    half = d // 2
    experts = ranks.shape[0]
    loads = [
        pltpu.make_async_copy(far, near, sems.at[k])
        for k, (far, near) in enumerate(((ids_far, ids), (rows_far, rows), (gain_far, gain)))
    ]
    for load in loads:
        load.start()
    ahead = (iota((tokens, tokens), 0) < iota((tokens, tokens), 1)).astype(f32).astype(bf16)
    expert = iota((experts, tokens), 0)
    loads[0].wait()
    chosen = (ids[0:1, :] == expert) | (ids[1:2, :] == expert)
    count = mm(chosen.astype(f32).astype(bf16), ahead)
    rank = jnp.where(chosen, count, -1.0)
    ranks[...] = rank
    _, slots, part = made.shape
    row = iota((experts, 8, tokens), 1)
    held = rank[:, None, :]

    def placing(hit):
        return hit.astype(f32).reshape(slots, tokens).astype(bf16)

    late = held == ((row & 3) + 8).astype(f32)
    places[0] = placing(held == row.astype(f32))
    places[1] = placing(late & (row < 4))
    places[2] = placing(late & (row >= 4))
    loads[1].wait()
    x = rows[...].astype(f32)
    mean = jnp.mean(x * x, axis=-1, keepdims=True)
    loads[2].wait()
    xn = (x * lax.rsqrt(mean + norm_eps) * gain[...]).astype(bf16)
    stores = []

    def send(step, values):
        made[step] = values.astype(bf16)
        stores.append(
            pltpu.make_async_copy(
                made.at[step], out.at[:, pl.ds(step * part, part)], out_sems.at[step]
            )
        )
        stores[-1].start()

    early = d // part
    for step in range(early):
        send(step, mm(places[0], xn[:, step * part : (step + 1) * part]))
    for step in range(half // part):
        left = xn[:, step * part : (step + 1) * part]
        right = xn[:, half + step * part : half + (step + 1) * part]
        send(early + step, mm(places[1], left) + mm(places[2], right))
    for store in stores:
        store.wait()


def silu_mul(gate, upper):
    return (gate / (1.0 + jnp.exp(-gate)) * upper).astype(bf16)


def ffn_body(x_far, wg, wu_far, wd_far, out, x, wu, wd, made, in_sems, sems):
    d, _ = wg.shape
    half = d // 2
    slots = x.shape[0]
    pieces = (
        (x_far.at[:, pl.ds(d, half)], x.at[:, pl.ds(d, half)]),
        (x_far.at[:, pl.ds(0, d)], x.at[:, pl.ds(0, d)]),
        (wu_far, wu),
        (wd_far, wd),
    )
    loads = [
        pltpu.make_async_copy(far, near, in_sems.at[k]) for k, (far, near) in enumerate(pieces)
    ]
    for load in loads:
        load.start()
    pairs = slots // 16

    def crossed(left, right):
        upper = (iota((1, 8, 1), 1) & 4) == 0
        return (
            jnp.where(upper, left, pltpu.roll(right, 4, 1)),
            jnp.where(upper, pltpu.roll(left, 4, 1), right),
        )

    loads[0].wait()
    x4 = x[:, d:].astype(f32).reshape(pairs, 2, 8, half)
    top, bottom = crossed(x4[:, 0], x4[:, 1])
    top = top.reshape(pairs * 8, half).astype(bf16)
    bottom = bottom.reshape(pairs * 8, half).astype(bf16)
    gate4 = mm(top, wg[:half, :]) + mm(bottom, wg[half:, :])
    loads[1].wait()
    x8 = x[:, :d]
    gate8 = mm(x8, wg[...])
    loads[2].wait()
    hidden4 = silu_mul(gate4, mm(top, wu[:half, :]) + mm(bottom, wu[half:, :]))
    hidden8 = silu_mul(gate8, mm(x8, wu[...]))
    loads[3].wait()
    part = made.shape[2]
    stores = []

    def send(step, values):
        made[step] = values.astype(bf16)
        stores.append(
            pltpu.make_async_copy(
                made.at[step], out.at[:, pl.ds(step * part, part)], sems.at[step]
            )
        )
        stores[-1].start()

    early = d // part
    for step in range(early):
        send(step, mm(hidden8, wd[:, step * part : (step + 1) * part]))
    for step in range(half // part):
        cols = slice(step * part, (step + 1) * part)
        far = slice(half + step * part, half + (step + 1) * part)
        left = mm(hidden4, wd[:, cols]).reshape(pairs, 8, part)
        right = mm(hidden4, wd[:, far]).reshape(pairs, 8, part)
        both = jnp.stack(crossed(left, right), axis=1)
        send(early + step, both.reshape(slots, part))
    for store in stores:
        store.wait()


def combine_body(ids, prob, scores, ranks, back, out):
    rank = ranks[...]
    experts, tokens = rank.shape
    s0, s1 = scores[0:1, :], scores[1:2, :]
    top = jnp.maximum(s0, s1)
    e0, e1 = jnp.exp(s0 - top), jnp.exp(s1 - top)
    both = e0 + e1
    w0, w1 = prob[...] * (e0 / both), prob[...] * (e1 / both)
    expert = iota((experts, tokens), 0)
    share = jnp.where(ids[0:1, :] == expert, w0, 0.0) + jnp.where(ids[1:2, :] == expert, w1, 0.0)
    row = iota((experts, 8, tokens), 1)

    def placed(hit):
        at = jnp.where(hit, share[:, None, :], 0.0).reshape(experts * 8, tokens)
        return at.T.astype(bf16)

    early = placed(rank[:, None, :] == row.astype(f32))
    hit = rank[:, None, :] == ((row & 3) + 8).astype(f32)
    half = out.shape[1] // 2
    late = back[:, 2 * half :]
    for h in range(2):
        cols = slice(h * half, (h + 1) * half)
        extra = mm(placed(hit & ((row >> 2) == h)), late)
        out[:, cols] = (mm(early, back[:, cols]) + extra).astype(bf16)


def running_keep(forget, boosts):
    x = forget[...]
    keep = boosts[...] - (jnp.maximum(-x, 0.0) + jnp.log1p(jnp.exp(-jnp.abs(x))))
    length = keep.shape[1]
    pieces = jnp.concatenate([*thirds(keep), jnp.zeros((5, length), f32)], axis=0).astype(bf16)
    upto = (iota((length, length), 0) <= iota((length, length), 1)).astype(f32).astype(bf16)
    return jnp.sum(mm(pieces, upto), axis=0, keepdims=True)


def side_rows(normer, total, peak):
    width = normer.shape[1]
    hi = normer.astype(bf16).astype(f32)
    lane = iota((1, width), 1)
    info = jnp.zeros((1, width), f32)
    for at, piece in enumerate((*thirds(total), *thirds(peak))):
        info = jnp.where(lane == at, piece, info)
    return jnp.concatenate([hi, normer - hi, info, jnp.zeros((5, width), f32)], axis=0)


def read_side(side):
    normer = side[0:1, :] + side[1:2, :]
    info = side[2:3, :]
    total = info[:, 0:1] + info[:, 1:2] + info[:, 2:3]
    peak = info[:, 3:4] + info[:, 4:5] + info[:, 5:6]
    return normer, total, peak


def summary_body(keys, values, gates, forget, boosts, out, rest):
    b = running_keep(forget, boosts)
    length = b.shape[1]
    width = keys.shape[1]
    last = b[:, length - 1 : length]
    gap = last - b + gates[...]
    peak = jnp.max(gap, axis=1, keepdims=True)
    spread = jnp.exp(gap - peak) * (width**-0.5)
    k = keys[...]
    scaled = (values[...].astype(f32).T * spread).astype(bf16)
    half = width // 2
    memory = mm(scaled, k).astype(bf16)
    out[:half, :] = memory[:half]
    rest[...] = memory[half:]
    hi, lo = halves(spread)
    two = jnp.concatenate([hi.astype(f32), lo.astype(f32), jnp.zeros((6, length), f32)], axis=0)
    normer = jnp.sum(mm(two.astype(bf16), k), axis=0, keepdims=True)
    out[half:, :] = side_rows(normer, last, peak).astype(bf16)


def weighted(pieces, logs, floor):
    stabil = floor
    for level in logs:
        stabil = jnp.maximum(stabil, level)
    memory, normer = None, None
    for (piece, n), level in zip(pieces, logs):
        factor = jnp.exp(level - stabil)
        memory = factor * piece if memory is None else memory + factor * piece
        normer = factor * n if normer is None else normer + factor * n
    return memory, normer, stabil


def before(mine, totals, peaks):
    logs, kept = [], []
    floor = jnp.full((1, 1), floor_log, f32)
    for j in range(len(totals)):
        level = peaks[j]
        for l in range(j + 1, len(totals)):
            level = level + jnp.where(l < mine, totals[l], 0.0)
        kept.append(j < mine)
        logs.append(jnp.where(j < mine, level, floor))
    return logs, kept


def masked(kept, pieces):
    return [(jnp.where(k, c, 0.0), jnp.where(k, n, 0.0)) for k, (c, n) in zip(kept, pieces)]


def plane_body(where, got, more, out, own, small, whole_memory):
    mine = where[1]
    width = got.shape[2]
    half = width // 2
    count = got.shape[0]
    pieces, totals, peaks = [], [], []
    for j in range(count):
        normer, total, peak = read_side(got[j, half:, :].astype(f32))
        memory = jnp.concatenate([got[j, :half, :], more[j]], axis=0).astype(f32)
        pieces.append((memory, normer))
        totals.append(total)
        peaks.append(peak)
    logs = []
    for j in range(count):
        level = peaks[j]
        for l in range(j + 1, count):
            level = level + totals[l]
        logs.append(level)
    memory, normer, stabil = weighted(pieces, logs, logs[0])
    everything = totals[0]
    for total in totals[1:]:
        everything = everything + total
    whole_memory[...] = memory
    part = width // count
    out[:part, :] = whole_memory[pl.ds(pl.multiple_of(mine * part, 8), part), :].astype(bf16)
    out[part:, :] = side_rows(normer, everything, stabil).astype(bf16)
    logs, kept = before(mine, totals, peaks)
    memory, normer, stabil = weighted(
        masked(kept, pieces), logs, jnp.full((1, 1), floor_log, f32)
    )
    own[...] = memory
    passed = jnp.zeros((1, 1), f32)
    for l in range(count):
        passed = passed + jnp.where(l < mine, totals[l], 0.0)
    small[0:1, :] = normer
    small[1:2, :] = jnp.broadcast_to(stabil, (1, width))
    small[2:3, :] = jnp.broadcast_to(passed, (1, width))
    small[3:8, :] = jnp.zeros((5, width), f32)


def line_body(where, *refs):
    got, (out, small) = refs[:-2], refs[-2:]
    mine = where[0]
    part, width = out.shape
    floor = jnp.full((1, 1), floor_log, f32)
    passed = jnp.zeros((1, 1), f32)
    pieces, logs, kept = [], [], []
    for step, piece in enumerate(got):
        normer, total, peak = read_side(piece[part:, :].astype(f32))
        near = step < mine
        pieces.append((piece[:part, :].astype(f32), normer))
        logs.append(jnp.where(near, peak + passed, floor))
        kept.append(near)
        passed = passed + jnp.where(near, total, 0.0)
    memory, normer, stabil = weighted(masked(kept, pieces), logs, floor)
    out[...] = memory.astype(bf16)
    small[0:1, :] = normer
    small[1:2, :] = jnp.broadcast_to(stabil, (1, width))
    small[2:8, :] = jnp.zeros((6, width), f32)


def cell_body(query, keys, values, gates, forget, boosts, state, line, own, near, scale, out):
    b = running_keep(forget, boosts)
    length = b.shape[1]
    width = keys.shape[1]
    b_col = jnp.broadcast_to(b, (128, length)).T
    far_log = near[2:3, 0:1] + line[1:2, 0:1]
    near_log = near[1:2, 0:1]
    stabil = jnp.maximum(far_log, near_log)
    far, close = jnp.exp(far_log - stabil), jnp.exp(near_log - stabil)
    normer = far * line[0:1, :] + close * near[0:1, :]
    memory = (far * state[...].astype(f32) + close * own[...]).astype(bf16)
    source = gates[...] - b
    block = 128
    for start in range(0, length, block):
        upto = start + block
        rows = slice(start, upto)
        q = query[rows, :]
        bt = b_col[rows, 0:1]
        decay = bt + source[:, :upto]
        seen = iota((block, upto), 1) <= iota((block, upto), 0) + start
        decay = jnp.where(seen, decay, -jnp.inf)
        carried = bt + stabil
        peak = jnp.maximum(carried, jnp.max(decay, axis=1, keepdims=True))
        across = jnp.exp(carried - peak)
        scores = mm_t(q, keys[:upto, :]) * (width**-0.5) * jnp.exp(decay - peak)
        den = jnp.sum(scores, axis=1, keepdims=True) + across * jnp.sum(
            q.astype(f32) * normer, axis=1, keepdims=True
        )
        num = mm(scores.astype(bf16), values[:upto, :]) + across * mm_t(q, memory)
        cell = num / jnp.maximum(jnp.abs(den), jnp.exp(-peak))
        out[rows, :] = (cell * scale[...]).astype(bf16)


def project_body(where, *refs):
    heads, (weight, gain, out) = refs[:-3], refs[-3:]
    count = len(heads)
    width = heads[0].shape[-1]
    total = None
    for step, head in enumerate(heads):
        source = lax.rem(where[2] + count - step, count)
        rows = weight[pl.ds(pl.multiple_of(source * width, width), width), :]
        product = mm(head[...], rows)
        total = product if total is None else total + product
    mean = jnp.mean(total * total, axis=-1, keepdims=True)
    out[...] = (total * lax.rsqrt(mean + norm_eps) * gain[...]).astype(bf16)


def exchanged(array, axes):
    return lax.all_to_all(array, axes, split_axis=0, concat_axis=0, tiled=True)


def after(array, *earlier):
    return lax.optimization_barrier((array, *earlier))[0]


def shards(
    query,
    keys,
    values,
    in_gates,
    forget,
    boosts,
    head_scale,
    out_weight,
    out_gain,
    rows,
    row_gain,
    ids,
    prob,
    scores,
    w_gate,
    w_up,
    w_down,
):
    devices = lax.axis_size(EP)
    positions, width = query.shape
    tokens, d = rows.shape
    hidden = w_gate.shape[2]
    slots = devices * 8
    line, plane = lax.axis_size("ep_0"), lax.axis_size(("ep_1", "ep_2"))
    planes = lax.axis_size("tp")
    ids_t = ids.T
    vm = pl.BlockSpec(memory_space=pltpu.VMEM)
    sm = pl.BlockSpec(memory_space=pltpu.SMEM)
    far_away = pl.BlockSpec(memory_space=pltpu.HBM)
    where = jnp.stack(
        [lax.axis_index("ep_0"), lax.axis_index(("ep_1", "ep_2")), lax.axis_index("tp")]
    ).astype(i32)

    out, ranks = call(
        build_body,
        (struct((slots, d + d // 2), bf16), struct((devices, tokens), f32)),
        ids_t,
        rows,
        row_gain.reshape(1, d),
        cost=4 * slots * tokens * d,
        specs=[far_away] * 3,
        out_specs=(far_away, vm),
        scratch=(
            pltpu.VMEM((2, tokens), i32),
            pltpu.VMEM((tokens, d), bf16),
            pltpu.VMEM((1, d), f32),
            pltpu.VMEM((3, slots, tokens), bf16),
            pltpu.VMEM((6, slots, d // 4), bf16),
            pltpu.SemaphoreType.DMA((3,)),
            pltpu.SemaphoreType.DMA((6,)),
        ),
        vmem=60,
    )
    got = exchanged(out.reshape(devices, 8, d + d // 2), EP)
    send, rest = call(
        summary_body,
        (struct((width // 2 + 8, width), bf16), struct((width // 2, width), bf16)),
        after(keys, out),
        values,
        in_gates,
        forget,
        boosts,
        cost=2 * positions * width * width * 4,
    )
    states = lax.all_gather(send, ("ep_1", "ep_2"))
    more = lax.all_gather(after(rest, states), ("ep_1", "ep_2"))
    plane_send, own, near = call(
        plane_body,
        (
            struct((width // plane + 8, width), bf16),
            struct((width, width), f32),
            struct((8, width), f32),
        ),
        where,
        states,
        more,
        cost=4 * plane * width * width * 100,
        scratch=(pltpu.VMEM((width, width), f32),),
        specs=[sm, vm, vm],
    )
    states = [
        lax.ppermute(plane_send, "ep_0", [(i, i + step) for i in range(line - step)])
        for step in range(1, line)
    ]
    send, far = call(
        line_body,
        (struct((width // plane, width), bf16), struct((8, width), f32)),
        where,
        *states,
        cost=4 * width * width * 100,
        specs=[sm] + [vm] * (line - 1),
    )
    answers = call(
        ffn_body,
        struct((slots, d + d // 2), bf16),
        after(got, plane_send).reshape(slots, d + d // 2),
        w_gate[0],
        w_up[0],
        w_down[0],
        cost=12 * slots * d * hidden,
        specs=[far_away, vm, far_away, far_away],
        out_specs=far_away,
        scratch=(
            pltpu.VMEM((slots, d + d // 2), bf16),
            pltpu.VMEM((d, hidden), bf16),
            pltpu.VMEM((hidden, d), bf16),
            pltpu.VMEM((6, slots, d // 4), bf16),
            pltpu.SemaphoreType.DMA((4,)),
            pltpu.SemaphoreType.DMA((6,)),
        ),
        vmem=50,
    )
    back = exchanged(answers.reshape(devices, 8, d + d // 2), EP)
    state = lax.all_gather(send, ("ep_1", "ep_2"), tiled=True)
    heads = call(
        cell_body,
        struct((positions, width), bf16),
        query,
        keys,
        values,
        in_gates,
        forget,
        boosts,
        state,
        far,
        own,
        near,
        head_scale.reshape(1, width),
        cost=2 * positions * positions * width * 40,
    )
    share = positions // planes
    me = where[2]
    pieces = []
    for step in range(planes):
        first = lax.rem(me + step, planes) * share
        piece = lax.dynamic_slice_in_dim(heads, first, share, 0)
        if step:
            ring = [(i, (i + step) % planes) for i in range(planes)]
            piece = lax.ppermute(piece, "tp", ring)
        pieces.append(piece)
    mixed_rows = call(
        project_body,
        struct((share, d), bf16),
        where,
        *pieces,
        out_weight,
        out_gain.reshape(1, d),
        cost=20 * positions * width * d,
        specs=[sm] + [vm] * (planes + 2),
    )
    routed_rows = call(
        combine_body,
        struct((tokens, d), bf16),
        ids_t,
        prob.reshape(1, tokens),
        scores.T,
        ranks,
        back.reshape(slots, d + d // 2),
        cost=12 * tokens * slots * d,
        vmem=16,
    )
    return (mixed_rows, routed_rows)


def solution(mesh):
    finer = Mesh(mesh.devices.reshape(8, 4, 2, mesh.shape["tp"]), ("ep_0", "ep_1", "ep_2", "tp"))
    in_specs = (
        P(EP, "tp"),
        P(EP, "tp"),
        P(EP, "tp"),
        P("tp", EP),
        P("tp", EP),
        P("tp", EP),
        P("tp"),
        P(),
        P(),
        P(EP_TP, None),
        P(),
        P(EP_TP, None),
        P(EP_TP),
        P(EP_TP, None),
        P(EP, None, None),
        P(EP, None, None),
        P(EP, None, None),
    )
    out_specs = (P(EP_TP, None), P(EP_TP, None))
    return jax.shard_map(
        shards, mesh=finer, in_specs=in_specs, out_specs=out_specs, check_vma=False
    )
```

```python
import jax
import jax.numpy as jnp
from jax import lax
from jax.experimental import pallas as pl
from jax.experimental.pallas import tpu as pltpu
from jax.sharding import Mesh
from jax.sharding import PartitionSpec as P

EP = ("ep_0", "ep_1", "ep_2")
EP_TP = ("ep_0", "ep_1", "ep_2", "tp")


floor_log = -1e30
norm_eps = 1e-06
f32, bf16, i32 = jnp.float32, jnp.bfloat16, jnp.int32


def iota(shape, dim):
    return lax.broadcasted_iota(i32, shape, dim)


def mm(a, b):
    return lax.dot_general(a, b, (((1,), (0,)), ((), ())), preferred_element_type=f32)


def mm_t(a, b):
    return lax.dot_general(a, b, (((1,), (1,)), ((), ())), preferred_element_type=f32)


def thirds(x):
    hi = x.astype(bf16).astype(f32)
    mid = (x - hi).astype(bf16).astype(f32)
    return hi, mid, (x - hi - mid).astype(bf16).astype(f32)


def halves(x):
    hi = x.astype(bf16)
    return hi, (x - hi.astype(f32)).astype(bf16)


def call(body, out_shape, *args, cost, scratch=(), specs=None, out_specs=None, grid=None, vmem=24):
    extra = {}
    if grid is not None:
        extra = dict(grid=grid, in_specs=specs, out_specs=out_specs)
    elif specs is not None:
        extra = dict(in_specs=specs)
        if out_specs is not None:
            extra["out_specs"] = out_specs
    return pl.pallas_call(
        body,
        out_shape=out_shape,
        scratch_shapes=list(scratch),
        compiler_params=pltpu.CompilerParams(vmem_limit_bytes=vmem << 20),
        cost_estimate=pl.CostEstimate(flops=cost, bytes_accessed=cost // 500, transcendentals=0),
        **extra,
    )(*args)


def struct(shape, dtype):
    return jax.ShapeDtypeStruct(shape, dtype)


def crossed(left, right):
    upper = (iota((1, 8, 1), 1) & 4) == 0
    return (
        jnp.where(upper, left, pltpu.roll(right, 4, 1)),
        jnp.where(upper, pltpu.roll(left, 4, 1), right),
    )


def unpacked(left, right):
    rows, part = left.shape
    pair = crossed(left.reshape(rows // 8, 8, part), right.reshape(rows // 8, 8, part))
    return jnp.stack(pair, axis=1).reshape(2 * rows, part)


def build_body(
    ids_far,
    rows_far,
    gain_far,
    out,
    ranks,
    ids,
    rows,
    gain,
    early_places,
    late_places,
    made,
    sems,
    out_sems,
):
    tokens, d = rows.shape
    half = d // 2
    experts = ranks.shape[0]
    loads = [
        pltpu.make_async_copy(far, near, sems.at[k])
        for k, (far, near) in enumerate(((ids_far, ids), (rows_far, rows), (gain_far, gain)))
    ]
    for load in loads:
        load.start()
    ahead = (iota((tokens, tokens), 0) < iota((tokens, tokens), 1)).astype(f32).astype(bf16)
    expert = iota((experts, tokens), 0)
    loads[0].wait()
    chosen = (ids[0:1, :] == expert) | (ids[1:2, :] == expert)
    count = mm(chosen.astype(f32).astype(bf16), ahead)
    rank = jnp.where(chosen, count, -1.0)
    ranks[...] = rank
    _, slots, part = made.shape
    held = rank[:, None, :]
    row = iota((experts, 8, tokens), 1).astype(f32)
    early_places[...] = (held == row).astype(f32).reshape(slots, tokens).astype(bf16)
    pairs = experts // 2
    held = held.reshape(pairs, 2, 1, tokens)
    row = iota((pairs, 8, tokens), 1)
    held = jnp.where(row < 4, held[:, 0], held[:, 1])
    hit = held == ((row & 3) + 8).astype(f32)
    late_places[...] = hit.astype(f32).reshape(slots // 2, tokens).astype(bf16)
    loads[1].wait()
    x = rows[...].astype(f32)
    mean = jnp.mean(x * x, axis=-1, keepdims=True)
    loads[2].wait()
    xn = (x * lax.rsqrt(mean + norm_eps) * gain[...]).astype(bf16)
    stores = []

    def send(step, values):
        made[step] = values.astype(bf16)
        stores.append(
            pltpu.make_async_copy(
                made.at[step], out.at[:, pl.ds(step * part, part)], out_sems.at[step]
            )
        )
        stores[-1].start()

    early = d // part
    for step in range(half // part):
        left = xn[:, step * part : (step + 1) * part]
        right = xn[:, half + step * part : half + (step + 1) * part]
        send(early + step, unpacked(mm(late_places[...], left), mm(late_places[...], right)))
    for step in range(early):
        send(step, mm(early_places[...], xn[:, step * part : (step + 1) * part]))
    for store in stores:
        store.wait()


def silu_mul(gate, upper):
    return (gate / (1.0 + jnp.exp(-gate)) * upper).astype(bf16)


def ffn_body(x_far, wg, wu_far, wd_far, out, x, wu, wd, made, in_sems, sems):
    d, _ = wg.shape
    half = d // 2
    slots = x.shape[0]
    pieces = (
        (x_far.at[:, pl.ds(0, d)], x.at[:, pl.ds(0, d)]),
        (x_far.at[:, pl.ds(d, half)], x.at[:, pl.ds(d, half)]),
        (wu_far, wu),
        (wd_far, wd),
    )
    loads = [
        pltpu.make_async_copy(far, near, in_sems.at[k]) for k, (far, near) in enumerate(pieces)
    ]
    for load in loads:
        load.start()
    pairs = slots // 16

    loads[0].wait()
    loads[1].wait()
    x8 = x[:, :d]
    gate8 = mm(x8, wg[...])
    x4 = x[:, d:].astype(f32).reshape(pairs, 2, 8, half)
    top, bottom = crossed(x4[:, 0], x4[:, 1])
    top = top.reshape(pairs * 8, half).astype(bf16)
    bottom = bottom.reshape(pairs * 8, half).astype(bf16)
    gate4 = mm(top, wg[:half, :]) + mm(bottom, wg[half:, :])
    loads[2].wait()
    hidden4 = silu_mul(gate4, mm(top, wu[:half, :]) + mm(bottom, wu[half:, :]))
    hidden8 = silu_mul(gate8, mm(x8, wu[...]))
    loads[3].wait()
    part = made.shape[2]
    stores = []

    def send(step, values):
        made[step] = values.astype(bf16)
        stores.append(
            pltpu.make_async_copy(
                made.at[step], out.at[:, pl.ds(step * part, part)], sems.at[step]
            )
        )
        stores[-1].start()

    early = d // part
    for step in range(early):
        send(step, mm(hidden8, wd[:, step * part : (step + 1) * part]))
    for step in range(half // part):
        left = mm(hidden4, wd[:, step * part : (step + 1) * part])
        right = mm(hidden4, wd[:, half + step * part : half + (step + 1) * part])
        send(early + step, unpacked(left, right))
    for store in stores:
        store.wait()


def combine_body(ids, prob, scores, ranks, back, out):
    rank = ranks[...]
    experts, tokens = rank.shape
    s0, s1 = scores[0:1, :], scores[1:2, :]
    top = jnp.maximum(s0, s1)
    e0, e1 = jnp.exp(s0 - top), jnp.exp(s1 - top)
    both = e0 + e1
    w0, w1 = prob[...] * (e0 / both), prob[...] * (e1 / both)
    expert = iota((experts, tokens), 0)
    share = jnp.where(ids[0:1, :] == expert, w0, 0.0) + jnp.where(ids[1:2, :] == expert, w1, 0.0)
    row = iota((experts, 8, tokens), 1)

    def placed(hit):
        at = jnp.where(hit, share[:, None, :], 0.0).reshape(experts * 8, tokens)
        return at.T.astype(bf16)

    early = placed(rank[:, None, :] == row.astype(f32))
    hit = rank[:, None, :] == ((row & 3) + 8).astype(f32)
    half = out.shape[1] // 2
    late = back[:, 2 * half :]
    for h in range(2):
        cols = slice(h * half, (h + 1) * half)
        extra = mm(placed(hit & ((row >> 2) == h)), late)
        out[:, cols] = (mm(early, back[:, cols]) + extra).astype(bf16)


def running_keep(forget, boosts):
    x = forget[...]
    keep = boosts[...] - (jnp.maximum(-x, 0.0) + jnp.log1p(jnp.exp(-jnp.abs(x))))
    length = keep.shape[1]
    pieces = jnp.concatenate([*thirds(keep), jnp.zeros((5, length), f32)], axis=0).astype(bf16)
    upto = (iota((length, length), 0) <= iota((length, length), 1)).astype(f32).astype(bf16)
    return jnp.sum(mm(pieces, upto), axis=0, keepdims=True)


def side_rows(normer, total, peak):
    width = normer.shape[1]
    hi = normer.astype(bf16).astype(f32)
    lane = iota((1, width), 1)
    info = jnp.zeros((1, width), f32)
    for at, piece in enumerate((*thirds(total), *thirds(peak))):
        info = jnp.where(lane == at, piece, info)
    return jnp.concatenate([hi, normer - hi, info, jnp.zeros((5, width), f32)], axis=0)


def read_side(side):
    normer = side[0:1, :] + side[1:2, :]
    info = side[2:3, :]
    total = info[:, 0:1] + info[:, 1:2] + info[:, 2:3]
    peak = info[:, 3:4] + info[:, 4:5] + info[:, 5:6]
    return normer, total, peak


def summary_body(keys, values, gates, forget, boosts, out, rest):
    b = running_keep(forget, boosts)
    length = b.shape[1]
    width = keys.shape[1]
    last = b[:, length - 1 : length]
    gap = last - b + gates[...]
    peak = jnp.max(gap, axis=1, keepdims=True)
    spread = jnp.exp(gap - peak) * (width**-0.5)
    k = keys[...]
    scaled = (values[...].astype(f32).T * spread).astype(bf16)
    half = width // 2
    memory = mm(scaled, k).astype(bf16)
    out[:half, :] = memory[:half]
    rest[...] = memory[half:]
    hi, lo = halves(spread)
    two = jnp.concatenate([hi.astype(f32), lo.astype(f32), jnp.zeros((6, length), f32)], axis=0)
    normer = jnp.sum(mm(two.astype(bf16), k), axis=0, keepdims=True)
    out[half:, :] = side_rows(normer, last, peak).astype(bf16)


def weighted(pieces, logs, floor):
    stabil = floor
    for level in logs:
        stabil = jnp.maximum(stabil, level)
    memory, normer = None, None
    for (piece, n), level in zip(pieces, logs):
        factor = jnp.exp(level - stabil)
        memory = factor * piece if memory is None else memory + factor * piece
        normer = factor * n if normer is None else normer + factor * n
    return memory, normer, stabil


def before(mine, totals, peaks):
    logs, kept = [], []
    floor = jnp.full((1, 1), floor_log, f32)
    for j in range(len(totals)):
        level = peaks[j]
        for l in range(j + 1, len(totals)):
            level = level + jnp.where(l < mine, totals[l], 0.0)
        kept.append(j < mine)
        logs.append(jnp.where(j < mine, level, floor))
    return logs, kept


def masked(kept, pieces):
    return [(jnp.where(k, c, 0.0), jnp.where(k, n, 0.0)) for k, (c, n) in zip(kept, pieces)]


def plane_body(where, got, more, out, own, small, whole_memory):
    mine = where[1]
    width = got.shape[2]
    half = width // 2
    count = got.shape[0]
    pieces, totals, peaks = [], [], []
    for j in range(count):
        normer, total, peak = read_side(got[j, half:, :].astype(f32))
        memory = jnp.concatenate([got[j, :half, :], more[j]], axis=0).astype(f32)
        pieces.append((memory, normer))
        totals.append(total)
        peaks.append(peak)
    logs = []
    for j in range(count):
        level = peaks[j]
        for l in range(j + 1, count):
            level = level + totals[l]
        logs.append(level)
    memory, normer, stabil = weighted(pieces, logs, logs[0])
    everything = totals[0]
    for total in totals[1:]:
        everything = everything + total
    whole_memory[...] = memory
    part = width // count
    out[:part, :] = whole_memory[pl.ds(pl.multiple_of(mine * part, 8), part), :].astype(bf16)
    out[part:, :] = side_rows(normer, everything, stabil).astype(bf16)
    logs, kept = before(mine, totals, peaks)
    memory, normer, stabil = weighted(
        masked(kept, pieces), logs, jnp.full((1, 1), floor_log, f32)
    )
    own[...] = memory
    passed = jnp.zeros((1, 1), f32)
    for l in range(count):
        passed = passed + jnp.where(l < mine, totals[l], 0.0)
    small[0:1, :] = normer
    small[1:2, :] = jnp.broadcast_to(stabil, (1, width))
    small[2:3, :] = jnp.broadcast_to(passed, (1, width))
    small[3:8, :] = jnp.zeros((5, width), f32)


def line_body(where, *refs):
    got, (out, small) = refs[:-2], refs[-2:]
    mine = where[0]
    part, width = out.shape
    floor = jnp.full((1, 1), floor_log, f32)
    passed = jnp.zeros((1, 1), f32)
    pieces, logs, kept = [], [], []
    for step, piece in enumerate(got):
        normer, total, peak = read_side(piece[part:, :].astype(f32))
        near = step < mine
        pieces.append((piece[:part, :].astype(f32), normer))
        logs.append(jnp.where(near, peak + passed, floor))
        kept.append(near)
        passed = passed + jnp.where(near, total, 0.0)
    memory, normer, stabil = weighted(masked(kept, pieces), logs, floor)
    out[...] = memory.astype(bf16)
    small[0:1, :] = normer
    small[1:2, :] = jnp.broadcast_to(stabil, (1, width))
    small[2:8, :] = jnp.zeros((6, width), f32)


def cell_body(query, keys, values, gates, forget, boosts, state, line, own, near, scale, out):
    b = running_keep(forget, boosts)
    length = b.shape[1]
    width = keys.shape[1]
    b_col = jnp.broadcast_to(b, (128, length)).T
    far_log = near[2:3, 0:1] + line[1:2, 0:1]
    near_log = near[1:2, 0:1]
    stabil = jnp.maximum(far_log, near_log)
    far, close = jnp.exp(far_log - stabil), jnp.exp(near_log - stabil)
    normer = far * line[0:1, :] + close * near[0:1, :]
    memory = (far * state[...].astype(f32) + close * own[...]).astype(bf16)
    source = gates[...] - b
    block = 128
    for start in range(0, length, block):
        upto = start + block
        rows = slice(start, upto)
        q = query[rows, :]
        bt = b_col[rows, 0:1]
        decay = bt + source[:, :upto]
        seen = iota((block, upto), 1) <= iota((block, upto), 0) + start
        decay = jnp.where(seen, decay, -jnp.inf)
        carried = bt + stabil
        peak = jnp.maximum(carried, jnp.max(decay, axis=1, keepdims=True))
        across = jnp.exp(carried - peak)
        scores = mm_t(q, keys[:upto, :]) * (width**-0.5) * jnp.exp(decay - peak)
        den = jnp.sum(scores, axis=1, keepdims=True) + across * jnp.sum(
            q.astype(f32) * normer, axis=1, keepdims=True
        )
        num = mm(scores.astype(bf16), values[:upto, :]) + across * mm_t(q, memory)
        cell = num / jnp.maximum(jnp.abs(den), jnp.exp(-peak))
        out[rows, :] = (cell * scale[...]).astype(bf16)


def project_body(where, *refs):
    heads, (weight, gain, out) = refs[:-3], refs[-3:]
    count = len(heads)
    width = heads[0].shape[-1]
    total = None
    for step, head in enumerate(heads):
        source = lax.rem(where[2] + count - step, count)
        rows = weight[pl.ds(pl.multiple_of(source * width, width), width), :]
        product = mm(head[...], rows)
        total = product if total is None else total + product
    mean = jnp.mean(total * total, axis=-1, keepdims=True)
    out[...] = (total * lax.rsqrt(mean + norm_eps) * gain[...]).astype(bf16)


def exchanged(array, axes):
    return lax.all_to_all(array, axes, split_axis=0, concat_axis=0, tiled=True)


def after(array, *earlier):
    return lax.optimization_barrier((array, *earlier))[0]


def shards(
    query,
    keys,
    values,
    in_gates,
    forget,
    boosts,
    head_scale,
    out_weight,
    out_gain,
    rows,
    row_gain,
    ids,
    prob,
    scores,
    w_gate,
    w_up,
    w_down,
):
    devices = lax.axis_size(EP)
    positions, width = query.shape
    tokens, d = rows.shape
    hidden = w_gate.shape[2]
    slots = devices * 8
    line, plane = lax.axis_size("ep_0"), lax.axis_size(("ep_1", "ep_2"))
    planes = lax.axis_size("tp")
    ids_t = ids.T
    vm = pl.BlockSpec(memory_space=pltpu.VMEM)
    sm = pl.BlockSpec(memory_space=pltpu.SMEM)
    far_away = pl.BlockSpec(memory_space=pltpu.HBM)
    where = jnp.stack(
        [lax.axis_index("ep_0"), lax.axis_index(("ep_1", "ep_2")), lax.axis_index("tp")]
    ).astype(i32)

    out, ranks = call(
        build_body,
        (struct((slots, d + d // 2), bf16), struct((devices, tokens), f32)),
        ids_t,
        rows,
        row_gain.reshape(1, d),
        cost=4 * slots * tokens * d,
        specs=[far_away] * 3,
        out_specs=(far_away, vm),
        scratch=(
            pltpu.VMEM((2, tokens), i32),
            pltpu.VMEM((tokens, d), bf16),
            pltpu.VMEM((1, d), f32),
            pltpu.VMEM((slots, tokens), bf16),
            pltpu.VMEM((slots // 2, tokens), bf16),
            pltpu.VMEM((6, slots, d // 4), bf16),
            pltpu.SemaphoreType.DMA((3,)),
            pltpu.SemaphoreType.DMA((6,)),
        ),
        vmem=60,
    )
    got = exchanged(out.reshape(devices, 8, d + d // 2), EP)
    send, rest = call(
        summary_body,
        (struct((width // 2 + 8, width), bf16), struct((width // 2, width), bf16)),
        after(keys, out),
        values,
        in_gates,
        forget,
        boosts,
        cost=2 * positions * width * width * 4,
    )
    states = lax.all_gather(send, ("ep_1", "ep_2"))
    more = lax.all_gather(after(rest, states), ("ep_1", "ep_2"))
    plane_send, own, near = call(
        plane_body,
        (
            struct((width // plane + 8, width), bf16),
            struct((width, width), f32),
            struct((8, width), f32),
        ),
        where,
        states,
        more,
        cost=4 * plane * width * width * 100,
        scratch=(pltpu.VMEM((width, width), f32),),
        specs=[sm, vm, vm],
    )
    states = [
        lax.ppermute(plane_send, "ep_0", [(i, i + step) for i in range(line - step)])
        for step in range(1, line)
    ]
    send, far = call(
        line_body,
        (struct((width // plane, width), bf16), struct((8, width), f32)),
        where,
        *states,
        cost=4 * width * width * 100,
        specs=[sm] + [vm] * (line - 1),
    )
    answers = call(
        ffn_body,
        struct((slots, d + d // 2), bf16),
        after(got, plane_send).reshape(slots, d + d // 2),
        w_gate[0],
        w_up[0],
        w_down[0],
        cost=12 * slots * d * hidden,
        specs=[far_away, vm, far_away, far_away],
        out_specs=far_away,
        scratch=(
            pltpu.VMEM((slots, d + d // 2), bf16),
            pltpu.VMEM((d, hidden), bf16),
            pltpu.VMEM((hidden, d), bf16),
            pltpu.VMEM((6, slots, d // 4), bf16),
            pltpu.SemaphoreType.DMA((4,)),
            pltpu.SemaphoreType.DMA((6,)),
        ),
        vmem=50,
    )
    back = exchanged(answers.reshape(devices, 8, d + d // 2), EP)
    state = lax.all_gather(send, ("ep_1", "ep_2"), tiled=True)
    heads = call(
        cell_body,
        struct((positions, width), bf16),
        query,
        keys,
        values,
        in_gates,
        forget,
        boosts,
        state,
        far,
        own,
        near,
        head_scale.reshape(1, width),
        cost=2 * positions * positions * width * 40,
    )
    share = positions // planes
    me = where[2]
    pieces = []
    for step in range(planes):
        first = lax.rem(me + step, planes) * share
        piece = lax.dynamic_slice_in_dim(heads, first, share, 0)
        if step:
            ring = [(i, (i + step) % planes) for i in range(planes)]
            piece = lax.ppermute(piece, "tp", ring)
        pieces.append(piece)
    mixed_rows = call(
        project_body,
        struct((share, d), bf16),
        where,
        *pieces,
        out_weight,
        out_gain.reshape(1, d),
        cost=20 * positions * width * d,
        specs=[sm] + [vm] * (planes + 2),
    )
    routed_rows = call(
        combine_body,
        struct((tokens, d), bf16),
        ids_t,
        prob.reshape(1, tokens),
        scores.T,
        ranks,
        back.reshape(slots, d + d // 2),
        cost=12 * tokens * slots * d,
        vmem=16,
    )
    return (mixed_rows, routed_rows)


def solution(mesh):
    finer = Mesh(mesh.devices.reshape(8, 4, 2, mesh.shape["tp"]), ("ep_0", "ep_1", "ep_2", "tp"))
    in_specs = (
        P(EP, "tp"),
        P(EP, "tp"),
        P(EP, "tp"),
        P("tp", EP),
        P("tp", EP),
        P("tp", EP),
        P("tp"),
        P(),
        P(),
        P(EP_TP, None),
        P(),
        P(EP_TP, None),
        P(EP_TP),
        P(EP_TP, None),
        P(EP, None, None),
        P(EP, None, None),
        P(EP, None, None),
    )
    out_specs = (P(EP_TP, None), P(EP_TP, None))
    return jax.shard_map(
        shards, mesh=finer, in_specs=in_specs, out_specs=out_specs, check_vma=False
    )
```
